32 devices in a mesh: ra: 16 (over z, y, x), cb: 2 (over core).
Axes of the slice: x: 2, y: 2, z: 4, core: 2. Of those that a mesh axis runs over, the one named last changes fastest.
Arguments:
- activations: bfloat16 [768, 4096], P('ra', 'cb'), may hold values from -230 to 230
- gain_first: float32 [4096], P('cb'), may hold values from 0.1 to 1.9
- gate_weight: float32 [11264, 4096], P('ra', 'cb'), may hold values from -0.125 to 0.125
- gate_scale: float32 [11264], P('ra'), may hold values from 0.5 to 2
- up_weight: float32 [11264, 4096], P('ra', 'cb'), may hold values from -0.125 to 0.125
- up_scale: float32 [11264], P('ra'), may hold values from 0.5 to 2
- down_weight: float32 [11264, 4096], P('ra', 'cb'), may hold values from -0.0546875 to 0.0546875
- down_scale: float32 [4096], P('cb'), may hold values from 0.35 to 2.8
- gain_second: float32 [4096], P('cb'), may hold values from 0.1 to 1.9
Outputs:
- normed: bfloat16 [768, 4096], P('ra', 'cb')
The draws below stay inside these ranges and needn't reach their ends.
All inputs are finite; a program needn't handle non-finite values.
Results may differ from the reference program's by a relative error of at most 0.011.
Values may be sent and summed in bfloat16 or wider, within the bound.
A program may use at most 64 MiB of HBM per device.

```python
import math
import jax
import jax.numpy as jnp
from jax import lax

D = 4096
FF = 11264
TOKENS = 768


def draw_activations(key, part):
    first, second, third = jax.random.split(jax.random.fold_in(key, 17), 3)
    columns = jnp.arange(D, dtype=jnp.float32) / D
    column_factor = jnp.exp(jnp.log(4.0) * (columns - 0.5)) * jax.random.uniform(second, (D,), jnp.float32, 0.6, 1.4)
    base = jnp.clip(jax.random.normal(first, (TOKENS, D), jnp.float32), -5.0, 5.0)
    rows = jnp.exp(jax.random.uniform(third, (TOKENS, 1), jnp.float32, 0.0, jnp.log(10.0)))
    return (base * rows * column_factor).astype(jnp.bfloat16)


def draw_down_scale(key, part):
    columns = jnp.arange(D, dtype=jnp.float32) / D
    rising = jnp.exp(jnp.log(4.0) * (columns - 0.5))
    noise = jax.random.uniform(jax.random.fold_in(key, 29), (D,), jnp.float32, 0.7, 1.4)
    return rising * noise


def raised(drawn, stream_key, source, target, blocks, factor):
    owner, partner = [(jnp.arange(drawn.shape[position]) // (drawn.shape[position] // blocks)).reshape([-1 if axis == position else 1 for axis in range(drawn.ndim)]) for position in (source, target)]
    chosen = jax.random.permutation(stream_key, blocks)[partner]
    strong = (owner == chosen) | (owner == (partner + blocks // 2) % blocks)
    return jnp.where(strong, factor * drawn, drawn)


def block_levels(own_key, extent, pieces, low, largest):
    factor_of, own = 1.0, jax.random.fold_in(own_key, 6)
    for position, shards_of in pieces:
        draws = jnp.exp(jax.random.uniform(jax.random.fold_in(own, position), (shards_of,), jnp.float32, low / len(pieces), largest / len(pieces)))
        factor_of = factor_of * jnp.repeat(draws, extent[position] // shards_of).reshape([-1 if axis == position else 1 for axis in range(len(extent))])
    return factor_of


def centred(rng, extent, spread, reach, shards=(), held_as=jnp.bfloat16):
    entries = jax.random.normal(rng, extent, jnp.float32) * spread
    if len(shards) > 0:
        entries = block_levels(rng, extent, shards, -0.22, 0.18) * entries
    return jnp.clip(entries, min=-reach, max=reach).astype(held_as)


def bell_draw_with(rng, dims, width, most, cuts, heavy, kind=jnp.bfloat16):
    drawn = width * jax.random.normal(rng, dims, jnp.float32)
    if cuts:
        drawn = drawn * block_levels(rng, dims, cuts, -0.22, 0.18)
    return jnp.clip(raised(drawn, jax.random.fold_in(rng, 3), *heavy), -most, most).astype(kind)


def setup_inputs(seed: int = 0) -> dict:
    seeds = jax.random.split(jax.random.key(seed), 10)
    activations = draw_activations(jax.random.fold_in(seeds[9], 71), 0)
    gain_first = jnp.clip(1.0 + 0.18 * jax.random.normal(seeds[1], (D,), jnp.float32), 0.1, 1.9)
    gate_weight = bell_draw_with(seeds[2], (FF, D), D ** -0.5, 0.125, ((0, 16), (1, 2)), (1, 0, 16, 2.0), jnp.float32)
    gate_scale = jnp.clip(jnp.exp(math.log(2.0) - 1.3862944 * jax.random.uniform(seeds[3], (FF,), jnp.float32) ** block_levels(seeds[3], (FF,), ((0, 16),), -0.2, 0.2)), 0.5, 2.0)
    up_weight = bell_draw_with(seeds[4], (FF, D), D ** -0.5, 0.125, ((0, 16), (1, 2)), (1, 0, 16, 2.0), jnp.float32)
    up_scale = jnp.clip(jnp.exp(math.log(2.0) - 1.3862944 * jax.random.uniform(seeds[5], (FF,), jnp.float32) ** block_levels(seeds[5], (FF,), ((0, 16),), -0.2, 0.2)), 0.5, 2.0)
    down_weight = centred(seeds[6], (FF, D), FF ** -0.5, 0.0546875, ((0, 16), (1, 2)), jnp.float32)
    down_scale = draw_down_scale(jax.random.fold_in(seeds[9], 71), 0)
    gain_second = jnp.clip(1.0 + 0.18 * jax.random.normal(seeds[8], (D,), jnp.float32), 0.1, 1.9)
    return {"activations": activations, "gain_first": gain_first, "gate_weight": gate_weight, "gate_scale": gate_scale, "up_weight": up_weight, "up_scale": up_scale, "down_weight": down_weight, "down_scale": down_scale, "gain_second": gain_second}


EPS = 1e-06

def reference(activations, gain_first, gate_weight, gate_scale, up_weight, up_scale, down_weight, down_scale, gain_second):
    inputs = activations.astype(jnp.float32)
    rscale_first = lax.rsqrt(lax.optimization_barrier(jnp.mean(inputs * inputs, axis=1)) + EPS)[:, None]
    scaled = (inputs * gain_first).astype(jnp.bfloat16)
    gate_raw = jnp.dot(scaled, gate_weight.astype(jnp.bfloat16).T, preferred_element_type=jnp.float32)
    up_raw = jnp.dot(scaled, up_weight.astype(jnp.bfloat16).T, preferred_element_type=jnp.float32)
    gate = gate_raw * rscale_first * gate_scale
    up = up_raw * rscale_first * up_scale
    hidden = (jax.nn.silu(gate) * up).astype(jnp.bfloat16)
    mixed = jnp.dot(hidden, down_weight.astype(jnp.bfloat16), preferred_element_type=jnp.float32) * down_scale
    stream = 0.1 * inputs + mixed
    rscale_second = lax.rsqrt(lax.optimization_barrier(jnp.mean(stream * stream, axis=1)) + EPS)[:, None]
    return (stream * rscale_second * gain_second).astype(jnp.bfloat16)
```

```python
import functools

import jax
import jax.numpy as jnp
from jax import lax
from jax.experimental import pallas as pl
from jax.experimental.pallas import tpu as pltpu
from jax.sharding import PartitionSpec as P

EPS = 1e-06
MESH = pl.DeviceIdType.MESH
F32 = jnp.float32
BF16 = jnp.bfloat16


def flip(index, mask):
    bit = 1
    while bit <= mask:
        if mask & bit:
            index = index + (1 - 2 * ((index // bit) % 2)) * bit
        bit *= 2
    return index


def kernel(
    planes,
    features,
    x_hbm,
    gain_hbm,
    gate_hbm,
    gate_scale_hbm,
    up_hbm,
    up_scale_hbm,
    down_hbm,
    down_scale_hbm,
    gain2_hbm,
    out_ref,
    wide,
    gate_w,
    up_w,
    down_w,
    gain_ref,
    gate_scale_ref,
    up_scale_ref,
    down_scale_ref,
    gain2_ref,
    xg,
    scaled,
    hidden,
    part,
    ex_send,
    ex_recv,
    sq_send,
    sq_recv,
    keep_a,
    keep_b,
    send_a,
    send_b,
    recv_a,
    recv_b,
    send2_a,
    send2_b,
    recv2_a,
    recv2_b,
    far,
    own_sum,
    z_send,
    z_recv,
    last_send,
    last_recv,
    in_sem,
    w_sem,
    ssem,
    rsem,
    zs_sem,
    zr_sem,
):
    ra = lax.axis_index("ra")
    cb = lax.axis_index("cb")
    rows, width = xg.shape[2:]
    half = width // 2
    x_peer = (flip(ra, 1), cb)
    y_peer = (flip(ra, 2), cb)
    z_peers = [None] + [(flip(ra, 4 * k), cb) for k in range(1, planes)]
    core_peer = (ra, flip(cb, 1))
    halves = (pl.ds(0, half), pl.ds(half, half))
    first, second = halves

    barrier = pltpu.get_barrier_semaphore()
    peers = [x_peer, y_peer, core_peer] + z_peers[1:]
    for peer in peers:
        pl.semaphore_signal(barrier, inc=1, device_id=peer, device_id_type=MESH)
    own = pltpu.make_async_copy(x_hbm, xg.at[0, 0], in_sem.at[0])
    own.start()
    small = []
    for i, (src, dst) in enumerate(
        (
            (gain_hbm, gain_ref),
            (gate_scale_hbm, gate_scale_ref),
            (up_scale_hbm, up_scale_ref),
            (down_scale_hbm, down_scale_ref),
            (gain2_hbm, gain2_ref),
        )
    ):
        load = pltpu.make_async_copy(src, dst, in_sem.at[i + 1])
        load.start()
        small.append(load)
    loads = []
    for i, src in enumerate((gate_hbm, up_hbm, down_hbm)):
        load = pltpu.make_async_copy(src, wide.at[i], w_sem.at[i])
        load.start()
        loads.append(load)
    own.wait()
    pl.semaphore_wait(barrier, len(peers))

    copies = {}
    slots = []

    def send(name, k, src, dst, peer):
        slot = len(slots)
        slots.append(name)
        copy = pltpu.make_async_remote_copy(
            src_ref=src,
            dst_ref=dst,
            send_sem=ssem.at[slot],
            recv_sem=rsem.at[slot],
            device_id=peer,
            device_id_type=MESH,
        )
        copy.start()
        copies[name, k] = copy

    seen = set()

    def arrived(name, k):
        if (name, k) in seen:
            return
        seen.add((name, k))
        copies[name, k].wait_recv()

    def to_x(k, h):
        send(("gx", h), k, xg.at[k, 0, :, halves[h]], xg.at[k, 1, :, halves[h]], x_peer)

    def to_y(k, h):
        send(("gy", h), k, xg.at[k, 0, :, halves[h]], xg.at[k, 2, :, halves[h]], y_peer)

    level = ra // 4
    inner = level % 2 != level // 2
    relays = []

    def to_z(source, target, h, peer):
        slot = len(relays)
        copy = pltpu.make_async_remote_copy(
            src_ref=xg.at[source, 0, :, halves[h]],
            dst_ref=xg.at[target, 0, :, halves[h]],
            send_sem=zs_sem.at[slot],
            recv_sem=zr_sem.at[target, h],
            device_id=z_peers[peer],
            device_id_type=MESH,
        )
        copies[("z", h), target] = copy
        relays.append(copy)
        if source or peer != 1:
            pl.when(inner)(copy.start)
        else:
            copy.start()

    def spread(k, h):
        to_x(k, h)
        to_y(k, h)

    def at_z1(h):
        arrived(("z", h), 1)
        to_z(1, 2, h, 3)

    def at_z2(h):
        arrived(("z", h), 2)
        to_z(2, 3, h, 1)
        spread(2, h)

    def relay_z3(h):
        @pl.when(inner)
        def _():
            copies[("z", h), 3].wait_recv()

        to_z(3, 2, h, 1)

    def at_z3(h):
        @pl.when(jnp.logical_not(inner))
        def _():
            copies[("z", h), 3].wait_recv()

        spread(3, h)

    def across(h):
        arrived(("fx", "fy")[h], 0)
        send(("e", h), 1, xg.at[0, 3, :, halves[h]], xg.at[1, 3, :, halves[h]], z_peers[1])

    def forward_y(k):
        arrived(("gx", 1), k)
        send("fy", k, xg.at[k, 1, :, second], xg.at[k, 3, :, second], y_peer)

    def forward_x(k):
        arrived(("gy", 0), k)
        send("fx", k, xg.at[k, 2, :, first], xg.at[k, 3, :, first], x_peer)

    nt = (((1,), (1,)), ((), ()))

    def prepare(k):
        def slot(s):
            block = xg[k, s].astype(F32)
            squares = jnp.sum(block * block, axis=1, keepdims=True)
            sq_send[k, s] = jnp.broadcast_to(squares, (rows, 128))
            scaled[s] = (block * gain_ref[...]).astype(BF16)

        slot(0)
        arrived(("gx", 1), k)
        arrived(("gx", 0), k)
        slot(1)
        arrived(("gy", 0), k)
        arrived(("gy", 1), k)
        slot(2)
        if k == 1:
            arrived(("e", 1), 1)
            arrived(("e", 0), 1)
        else:
            arrived("fy", k)
            if k == 0:
                across(1)
            arrived("fx", k)
            if k == 0:
                across(0)
        slot(3)
        send("sq", k, sq_send.at[k], sq_recv.at[k], core_peer)

    def product(k, i):
        tokens = scaled[...].reshape(4 * rows, width)
        w = (gate_w, up_w)[i]
        product = lax.dot_general(tokens, w[...], nt, preferred_element_type=F32)
        part[k, i] = product
        ex_send[k, i] = product.astype(BF16)
        send(("ex", i), k, ex_send.at[k, i], ex_recv.at[k, i], core_peer)

    def activate(k):
        arrived("sq", k)
        arrived(("ex", 0), k)
        arrived(("ex", 1), k)
        for s in range(4):
            here = slice(s * rows, (s + 1) * rows)
            squares = (sq_send[k, s] + sq_recv[k, s])[:, :1]
            rscale = lax.rsqrt(squares / features + EPS)
            gate = (part[k, 0, here] + ex_recv[k, 0, here].astype(F32)) * rscale * gate_scale_ref[...][None, :]
            up = (part[k, 1, here] + ex_recv[k, 1, here].astype(F32)) * rscale * up_scale_ref[...][None, :]
            hidden[k, here] = (gate / (1.0 + jnp.exp(-gate)) * up).astype(BF16)

    def down_a(k):
        prod = jnp.dot(hidden[k], down_w[:, :half], preferred_element_type=F32)
        keep_a[k, 0] = prod[:rows]
        send_a[k, 0] = prod[rows : 2 * rows].astype(BF16)
        if k == 1:
            send2_a[k] = prod[2 * rows : 3 * rows].astype(BF16)
        else:
            keep_a[k, 1] = prod[2 * rows : 3 * rows]
        if k:
            send_a[k, 1] = prod[3 * rows :].astype(BF16)
        else:
            far[0] = prod[3 * rows :]

    def down_b(k):
        prod = jnp.dot(hidden[k], down_w[:, half:], preferred_element_type=F32)
        keep_b[k, 0] = prod[:rows]
        if k == 1:
            send2_b[k] = prod[rows : 2 * rows].astype(BF16)
        else:
            keep_b[k, 1] = prod[rows : 2 * rows]
        send_b[k, 0] = prod[2 * rows : 3 * rows].astype(BF16)
        if k:
            send_b[k, 1] = prod[3 * rows :].astype(BF16)
        else:
            far[1] = prod[3 * rows :]

    def one_a(k, d):
        send(("a1", d), k, send_a.at[k, d], recv_a.at[k, d], x_peer)

    def one_b(k, d):
        send(("b1", d), k, send_b.at[k, d], recv_b.at[k, d], y_peer)

    def down(k):
        activate(k)
        down_a(k)
        if k == 1:
            send(("r", 0), 1, send_a.at[1, 1], recv_a.at[1, 1], z_peers[1])
            one_a(1, 0)
            send("a2", 1, send2_a.at[1], recv2_a.at[1], y_peer)
        else:
            one_a(k, 1)
        down_b(k)
        if k == 1:
            send(("r", 1), 1, send_b.at[1, 1], recv_b.at[1, 1], z_peers[1])
            one_b(1, 0)
            send("b2", 1, send2_b.at[1], recv2_b.at[1], x_peer)
        else:
            one_b(k, 1)
            one_a(k, 0)
            one_b(k, 0)

    def merge():
        arrived(("r", 0), 1)
        send_a[0, 1] = (far[0] + recv_a[1, 1].astype(F32)).astype(BF16)
        one_a(0, 1)
        arrived(("r", 1), 1)
        send_b[0, 1] = (far[1] + recv_b[1, 1].astype(F32)).astype(BF16)
        one_b(0, 1)

    def two(k):
        arrived(("a1", 1), k)
        send2_a[k] = (keep_a[k, 1] + recv_a[k, 1].astype(F32)).astype(BF16)
        send("a2", k, send2_a.at[k], recv2_a.at[k], y_peer)
        arrived(("b1", 1), k)
        send2_b[k] = (keep_b[k, 1] + recv_b[k, 1].astype(F32)).astype(BF16)
        send("b2", k, send2_b.at[k], recv2_b.at[k], x_peer)

    def home(k):
        arrived(("a1", 0), k)
        arrived("a2", k)
        sum_a = keep_a[k, 0] + recv_a[k, 0].astype(F32) + recv2_a[k].astype(F32)
        if k:
            z_send[k, 0] = sum_a.astype(BF16)
            send(("zs", 0), k, z_send.at[k, 0], z_recv.at[k, 0], z_peers[k])
        arrived(("b1", 0), k)
        arrived("b2", k)
        sum_b = keep_b[k, 0] + recv_b[k, 0].astype(F32) + recv2_b[k].astype(F32)
        if k:
            z_send[k, 1] = sum_b.astype(BF16)
            send(("zs", 1), k, z_send.at[k, 1], z_recv.at[k, 1], z_peers[k])
            return
        own_sum[:, :half] = sum_a
        own_sum[:, half:] = sum_b

    def collect(k):
        for h in range(2):
            arrived(("zs", h), k)
            own_sum[:, halves[h]] += z_recv[k, h].astype(F32)

    def narrow(i, target):
        loads[i].wait()
        step = 64

        def body(j, carry):
            here = pl.ds(pl.multiple_of(j * step, step), step)
            target[here] = wide[i, here].astype(BF16)
            return carry

        lax.fori_loop(0, target.shape[0] // step, body, 0)

    for h in (1, 0):
        to_x(0, h)
        to_y(0, 1 - h)
        to_z(0, 1, h, 1)
    for h in (1, 0):
        to_z(0, 3, h, 3)
    narrow(0, gate_w)
    narrow(1, up_w)
    forward_y(0)
    forward_x(0)
    for h in (1, 0):
        relay_z3(h)
        at_z1(h)
        spread(1, h)
    for load in small:
        load.wait()
    prepare(0)
    at_z2(1)
    product(0, 0)
    at_z2(0)
    product(0, 1)
    at_z3(1)
    forward_y(2)
    at_z3(0)
    forward_x(2)

    narrow(2, down_w)
    activate(0)
    down_a(0)
    down_b(0)
    forward_y(3)

    prepare(2)
    forward_x(3)
    one_a(0, 0)
    one_b(0, 0)
    product(2, 0)
    product(2, 1)
    prepare(3)
    product(3, 0)
    down(2)
    product(3, 1)
    prepare(1)
    product(1, 0)
    two(2)
    down(3)
    product(1, 1)
    home(2)
    two(3)
    down(1)
    home(3)
    merge()
    home(1)
    two(0)
    home(0)
    collect(2)
    collect(1)
    collect(3)

    stream = 0.1 * xg[0, 0].astype(F32) + own_sum[...] * down_scale_ref[...]
    own_sum[...] = stream
    last_send[...] = jnp.broadcast_to(
        jnp.sum(stream * stream, axis=1, keepdims=True), last_send.shape
    )
    send("last", 0, last_send, last_recv, core_peer)
    arrived("last", 0)
    both = (last_send[...] + last_recv[...])[:, :1]
    rscale = lax.rsqrt(both / features + EPS)
    out_ref[...] = (own_sum[...] * rscale * gain2_ref[...]).astype(BF16)
    for (name, _), copy in copies.items():
        if name[0] != "z":
            copy.wait_send()
    for copy in relays[:2]:
        copy.wait_send()

    @pl.when(inner)
    def _():
        for copy in relays[2:]:
            copy.wait_send()


def fused(
    planes,
    activations,
    gain_first,
    gate_weight,
    gate_scale,
    up_weight,
    up_scale,
    down_weight,
    down_scale,
    gain_second,
):
    rows, width = activations.shape
    units = gate_weight.shape[0]
    half = width // 2
    group = 4 * rows
    n_copies = 24 * planes
    vmem = pl.BlockSpec(memory_space=pltpu.VMEM)
    hbm = pl.BlockSpec(memory_space=pl.ANY)
    scratch = [
        pltpu.VMEM((3, units, width), F32),
        pltpu.VMEM((units, width), BF16),
        pltpu.VMEM((units, width), BF16),
        pltpu.VMEM((units, width), BF16),
        pltpu.VMEM((1, width), F32),
        pltpu.VMEM((units,), F32),
        pltpu.VMEM((units,), F32),
        pltpu.VMEM((1, width), F32),
        pltpu.VMEM((1, width), F32),
        pltpu.VMEM((planes, 4, rows, width), BF16),
        pltpu.VMEM((4, rows, width), BF16),
        pltpu.VMEM((planes, group, units), BF16),
        pltpu.VMEM((planes, 2, group, units), F32),
        pltpu.VMEM((planes, 2, group, units), BF16),
        pltpu.VMEM((planes, 2, group, units), BF16),
        pltpu.VMEM((planes, 4, rows, 128), F32),
        pltpu.VMEM((planes, 4, rows, 128), F32),
        pltpu.VMEM((planes, 2, rows, half), F32),
        pltpu.VMEM((planes, 2, rows, half), F32),
        pltpu.VMEM((planes, 2, rows, half), BF16),
        pltpu.VMEM((planes, 2, rows, half), BF16),
        pltpu.VMEM((planes, 2, rows, half), BF16),
        pltpu.VMEM((planes, 2, rows, half), BF16),
        pltpu.VMEM((planes, rows, half), BF16),
        pltpu.VMEM((planes, rows, half), BF16),
        pltpu.VMEM((planes, rows, half), BF16),
        pltpu.VMEM((planes, rows, half), BF16),
        pltpu.VMEM((2, rows, half), F32),
        pltpu.VMEM((rows, width), F32),
        pltpu.VMEM((planes, 2, rows, half), BF16),
        pltpu.VMEM((planes, 2, rows, half), BF16),
        pltpu.VMEM((rows, 128), F32),
        pltpu.VMEM((rows, 128), F32),
        pltpu.SemaphoreType.DMA((6,)),
        pltpu.SemaphoreType.DMA((3,)),
        pltpu.SemaphoreType.DMA((n_copies,)),
        pltpu.SemaphoreType.DMA((n_copies,)),
        pltpu.SemaphoreType.DMA((10,)),
        pltpu.SemaphoreType.DMA((planes, 2)),
    ]
    return pl.pallas_call(
        functools.partial(kernel, planes, width * 2),
        out_shape=jax.ShapeDtypeStruct((rows, width), BF16),
        in_specs=[hbm] * 9,
        out_specs=vmem,
        scratch_shapes=scratch,
        compiler_params=pltpu.CompilerParams(
            collective_id=0, has_side_effects=True, vmem_limit_bytes=60 * 1024 * 1024
        ),
    )(
        activations,
        gain_first[None, :],
        gate_weight,
        gate_scale,
        up_weight,
        up_scale,
        down_weight,
        down_scale[None, :],
        gain_second[None, :],
    )


def plain(
    activations,
    gain_first,
    gate_weight,
    gate_scale,
    up_weight,
    up_scale,
    down_weight,
    down_scale,
    gain_second,
):
    inputs = activations.astype(F32)
    features = activations.shape[1] * lax.axis_size("cb")
    gate_local = gate_weight.astype(BF16)
    up_local = up_weight.astype(BF16)
    down_local = down_weight.astype(BF16)
    gathered = lax.all_gather(activations, "ra", axis=0, tiled=True)
    wide_rows = gathered.astype(F32)
    row_squares = jnp.sum(wide_rows * wide_rows, axis=1)
    scaled = (wide_rows * gain_first).astype(BF16)
    contract = (((1,), (1,)), ((), ()))
    squares = lax.psum(row_squares, "cb")
    gate_part = lax.dot_general(gate_local, scaled, contract, preferred_element_type=F32)
    up_part = lax.dot_general(up_local, scaled, contract, preferred_element_type=F32)
    gate_sum, up_sum = lax.psum((gate_part, up_part), "cb")
    rscale_first = lax.rsqrt(squares / features + EPS)[None, :]
    gate_full = gate_sum * rscale_first * gate_scale[:, None]
    up_full = up_sum * rscale_first * up_scale[:, None]
    hidden = (jax.nn.silu(gate_full) * up_full).astype(BF16)
    mixed = lax.dot_general(hidden, down_local, (((0,), (0,)), ((), ())), preferred_element_type=F32)
    summed = lax.psum_scatter(mixed, "ra", scatter_dimension=0, tiled=True)
    stream = 0.1 * inputs + summed * down_scale
    second = lax.psum(jnp.sum(stream * stream, axis=1), "cb")
    rscale_second = lax.rsqrt(second / features + EPS)[:, None]
    return (stream * rscale_second * gain_second).astype(BF16)


def solution(mesh):
    placed = (
        P("ra", "cb"),
        P("cb"),
        P("ra", "cb"),
        P("ra"),
        P("ra", "cb"),
        P("ra"),
        P("ra", "cb"),
        P("cb"),
        P("cb"),
    )
    planes = mesh.shape["ra"] // 4
    paired = mesh.shape["cb"] == 2 and planes == 4
    body = functools.partial(fused, planes) if paired else plain
    return jax.shard_map(
        body, mesh=mesh, in_specs=placed, out_specs=P("ra", "cb"), check_vma=False
    )
```

```python
import functools

import jax
import jax.numpy as jnp
from jax import lax
from jax.experimental import pallas as pl
from jax.experimental.pallas import tpu as pltpu
from jax.sharding import PartitionSpec as P

EPS = 1e-06
MESH = pl.DeviceIdType.MESH
F32 = jnp.float32
BF16 = jnp.bfloat16


def flip(index, mask):
    bit = 1
    while bit <= mask:
        if mask & bit:
            index = index + (1 - 2 * ((index // bit) % 2)) * bit
        bit *= 2
    return index


def kernel(
    planes,
    features,
    x_hbm,
    gain_hbm,
    gate_hbm,
    gate_scale_hbm,
    up_hbm,
    up_scale_hbm,
    down_hbm,
    down_scale_hbm,
    gain2_hbm,
    out_ref,
    wide,
    gate_w,
    up_w,
    down_w,
    gain_ref,
    gate_scale_ref,
    up_scale_ref,
    down_scale_ref,
    gain2_ref,
    xg,
    scaled,
    hidden,
    part,
    ex_send,
    ex_recv,
    sq_send,
    sq_recv,
    keep_a,
    keep_b,
    send_a,
    send_b,
    recv_a,
    recv_b,
    send2_a,
    send2_b,
    recv2_a,
    recv2_b,
    far,
    own_sum,
    z_send,
    z_recv,
    last_send,
    last_recv,
    in_sem,
    w_sem,
    ssem,
    rsem,
    zs_sem,
    zr_sem,
):
    ra = lax.axis_index("ra")
    cb = lax.axis_index("cb")
    rows, width = xg.shape[2:]
    half = width // 2
    x_peer = (flip(ra, 1), cb)
    y_peer = (flip(ra, 2), cb)
    z_peers = [None] + [(flip(ra, 4 * k), cb) for k in range(1, planes)]
    core_peer = (ra, flip(cb, 1))
    halves = (pl.ds(0, half), pl.ds(half, half))
    first, second = halves

    barrier = pltpu.get_barrier_semaphore()
    peers = [x_peer, y_peer, core_peer] + z_peers[1:]
    for peer in peers:
        pl.semaphore_signal(barrier, inc=1, device_id=peer, device_id_type=MESH)
    own = pltpu.make_async_copy(x_hbm, xg.at[0, 0], in_sem.at[0])
    own.start()
    small = []
    for i, (src, dst) in enumerate(
        (
            (gain_hbm, gain_ref),
            (gate_scale_hbm, gate_scale_ref),
            (up_scale_hbm, up_scale_ref),
            (down_scale_hbm, down_scale_ref),
            (gain2_hbm, gain2_ref),
        )
    ):
        load = pltpu.make_async_copy(src, dst, in_sem.at[i + 1])
        load.start()
        small.append(load)
    loads = []
    for i, src in enumerate((gate_hbm, up_hbm, down_hbm)):
        load = pltpu.make_async_copy(src, wide.at[i], w_sem.at[i])
        load.start()
        loads.append(load)
    own.wait()
    pl.semaphore_wait(barrier, len(peers))

    copies = {}
    slots = []

    def send(name, k, src, dst, peer):
        slot = len(slots)
        slots.append(name)
        copy = pltpu.make_async_remote_copy(
            src_ref=src,
            dst_ref=dst,
            send_sem=ssem.at[slot],
            recv_sem=rsem.at[slot],
            device_id=peer,
            device_id_type=MESH,
        )
        copy.start()
        copies[name, k] = copy

    seen = set()

    def arrived(name, k):
        if (name, k) in seen:
            return
        seen.add((name, k))
        copies[name, k].wait_recv()

    def to_x(k, h):
        send(("gx", h), k, xg.at[k, 0, :, halves[h]], xg.at[k, 1, :, halves[h]], x_peer)

    def to_y(k, h):
        send(("gy", h), k, xg.at[k, 0, :, halves[h]], xg.at[k, 2, :, halves[h]], y_peer)

    level = ra // 4
    inner = level % 2 != level // 2
    relays = []

    def to_z(source, target, h, peer):
        slot = len(relays)
        copy = pltpu.make_async_remote_copy(
            src_ref=xg.at[source, 0, :, halves[h]],
            dst_ref=xg.at[target, 0, :, halves[h]],
            send_sem=zs_sem.at[slot],
            recv_sem=zr_sem.at[target, h],
            device_id=z_peers[peer],
            device_id_type=MESH,
        )
        copies[("z", h), target] = copy
        relays.append(copy)
        if source or peer != 1:
            pl.when(inner)(copy.start)
        else:
            copy.start()

    def spread(k, h):
        to_x(k, h)
        to_y(k, h)

    def at_z1(h):
        arrived(("z", h), 1)
        to_z(1, 2, h, 3)

    def at_z2(h):
        arrived(("z", h), 2)
        to_z(2, 3, h, 1)
        spread(2, h)

    def relay_z3(h):
        @pl.when(inner)
        def _():
            copies[("z", h), 3].wait_recv()

        to_z(3, 2, h, 1)

    def at_z3(h):
        @pl.when(jnp.logical_not(inner))
        def _():
            copies[("z", h), 3].wait_recv()

        spread(3, h)

    def forward_y(k):
        arrived(("gx", 1), k)
        send("fy", k, xg.at[k, 1, :, second], xg.at[k, 3, :, second], y_peer)

    def forward_x(k):
        arrived(("gy", 0), k)
        send("fx", k, xg.at[k, 2, :, first], xg.at[k, 3, :, first], x_peer)

    nt = (((1,), (1,)), ((), ()))

    def prepare(k):
        def slot(s):
            block = xg[k, s].astype(F32)
            squares = jnp.sum(block * block, axis=1, keepdims=True)
            sq_send[k, s] = jnp.broadcast_to(squares, (rows, 128))
            scaled[k, s] = (block * gain_ref[...]).astype(BF16)

        slot(0)
        arrived(("gx", 1), k)
        arrived(("gx", 0), k)
        slot(1)
        arrived(("gy", 0), k)
        arrived(("gy", 1), k)
        slot(2)
        arrived("fy", k)
        arrived("fx", k)
        slot(3)
        send("sq", k, sq_send.at[k], sq_recv.at[k], core_peer)

    def product(k, i):
        tokens = scaled[k].reshape(4 * rows, width)
        w = (gate_w, up_w)[i]
        product = lax.dot_general(tokens, w[...], nt, preferred_element_type=F32)
        part[k, i] = product
        ex_send[k, i] = product.astype(BF16)
        send(("ex", i), k, ex_send.at[k, i], ex_recv.at[k, i], core_peer)

    def activate(k):
        arrived("sq", k)
        arrived(("ex", 0), k)
        arrived(("ex", 1), k)
        for s in range(4):
            here = slice(s * rows, (s + 1) * rows)
            squares = (sq_send[k, s] + sq_recv[k, s])[:, :1]
            rscale = lax.rsqrt(squares / features + EPS)
            gate = (part[k, 0, here] + ex_recv[k, 0, here].astype(F32)) * rscale * gate_scale_ref[...][None, :]
            up = (part[k, 1, here] + ex_recv[k, 1, here].astype(F32)) * rscale * up_scale_ref[...][None, :]
            hidden[k, here] = (gate / (1.0 + jnp.exp(-gate)) * up).astype(BF16)

    def down_a(k):
        prod = jnp.dot(hidden[k], down_w[:, :half], preferred_element_type=F32)
        keep_a[k, 0] = prod[:rows]
        send_a[k, 0] = prod[rows : 2 * rows].astype(BF16)
        if k == 1:
            send2_a[k] = prod[2 * rows : 3 * rows].astype(BF16)
        else:
            keep_a[k, 1] = prod[2 * rows : 3 * rows]
        if k:
            send_a[k, 1] = prod[3 * rows :].astype(BF16)
        else:
            far[0] = prod[3 * rows :]

    def down_b(k):
        prod = jnp.dot(hidden[k], down_w[:, half:], preferred_element_type=F32)
        keep_b[k, 0] = prod[:rows]
        send_b[k, 0] = prod[2 * rows : 3 * rows].astype(BF16)
        if k == 1:
            send2_b[k] = prod[rows : 2 * rows].astype(BF16)
        else:
            keep_b[k, 1] = prod[rows : 2 * rows]
        if k:
            send_b[k, 1] = prod[3 * rows :].astype(BF16)
        else:
            far[1] = prod[3 * rows :]

    def one_a(k, d):
        send(("a1", d), k, send_a.at[k, d], recv_a.at[k, d], x_peer)

    def one_b(k, d):
        send(("b1", d), k, send_b.at[k, d], recv_b.at[k, d], y_peer)

    def cross_a():
        send(("r", 0), 1, send_a.at[1, 1], recv_a.at[1, 1], z_peers[1])
        one_a(1, 0)
        send("a2", 1, send2_a.at[1], recv2_a.at[1], y_peer)

    def cross_b():
        send(("r", 1), 1, send_b.at[1, 1], recv_b.at[1, 1], z_peers[1])
        one_b(1, 0)
        send("b2", 1, send2_b.at[1], recv2_b.at[1], x_peer)

    def merge_a():
        arrived(("r", 0), 1)
        send_a[0, 1] = (far[0] + recv_a[1, 1].astype(F32)).astype(BF16)
        one_a(0, 1)

    def merge_b():
        arrived(("r", 1), 1)
        send_b[0, 1] = (far[1] + recv_b[1, 1].astype(F32)).astype(BF16)
        one_b(0, 1)

    def two_a(k):
        arrived(("a1", 1), k)
        send2_a[k] = (keep_a[k, 1] + recv_a[k, 1].astype(F32)).astype(BF16)
        send("a2", k, send2_a.at[k], recv2_a.at[k], y_peer)

    def two_b(k):
        arrived(("b1", 1), k)
        send2_b[k] = (keep_b[k, 1] + recv_b[k, 1].astype(F32)).astype(BF16)
        send("b2", k, send2_b.at[k], recv2_b.at[k], x_peer)

    def home(k, h, mine):
        if k == 0:
            own_sum[:, halves[h]] = mine
            return
        if k == 3:
            arrived(("zs", h), 2)
            mine = mine + z_recv[2, h].astype(F32)
        peer = z_peers[1 if k == 2 else k]
        z_send[k, h] = mine.astype(BF16)
        send(("zs", h), k, z_send.at[k, h], z_recv.at[k, h], peer)

    def home_a(k):
        arrived(("a1", 0), k)
        arrived("a2", k)
        home(k, 0, keep_a[k, 0] + recv_a[k, 0].astype(F32) + recv2_a[k].astype(F32))

    def home_b(k):
        arrived(("b1", 0), k)
        arrived("b2", k)
        home(k, 1, keep_b[k, 0] + recv_b[k, 0].astype(F32) + recv2_b[k].astype(F32))

    def collect(k):
        for h in range(2):
            arrived(("zs", h), k)
            own_sum[:, halves[h]] += z_recv[k, h].astype(F32)

    def narrow(i, target):
        loads[i].wait()
        step = 64

        def body(j, carry):
            here = pl.ds(pl.multiple_of(j * step, step), step)
            target[here] = wide[i, here].astype(BF16)
            return carry

        lax.fori_loop(0, target.shape[0] // step, body, 0)

    for h in (1, 0):
        to_x(0, h)
        to_y(0, 1 - h)
        to_z(0, 1, h, 1)
    for h in (1, 0):
        to_z(0, 3, h, 3)
    forward_x(0)
    forward_y(0)
    relay_z3(1)
    narrow(1, up_w)
    narrow(0, gate_w)
    at_z1(1)
    at_z1(0)
    spread(1, 0)
    relay_z3(0)
    at_z2(1)
    narrow(2, down_w)
    at_z2(0)
    for load in small:
        load.wait()
    prepare(0)
    product(0, 1)
    forward_x(2)
    forward_y(2)
    at_z3(0)
    at_z3(1)
    product(0, 0)
    prepare(2)
    activate(0)
    spread(1, 1)
    product(2, 1)
    forward_x(3)
    product(2, 0)
    down_a(0)
    forward_y(3)
    forward_x(1)
    forward_y(1)
    down_b(0)
    activate(2)
    down_b(2)
    one_b(2, 0)
    down_a(2)
    one_a(2, 1)
    one_a(2, 0)
    prepare(3)
    product(3, 1)
    one_b(2, 1)
    one_a(0, 0)
    product(3, 0)
    prepare(1)
    product(1, 1)
    one_b(0, 0)
    two_a(2)
    product(1, 0)
    activate(3)
    down_a(3)
    one_a(3, 1)
    down_b(3)
    one_b(3, 1)
    two_b(2)
    activate(1)
    one_a(3, 0)
    home_a(2)
    down_a(1)
    cross_a()
    two_a(3)
    down_b(1)
    two_b(3)
    one_b(3, 0)
    cross_b()
    home_b(2)
    home_a(1)
    home_a(3)
    merge_b()
    merge_a()
    home_b(3)
    home_b(1)
    two_a(0)
    two_b(0)
    home_b(0)
    home_a(0)
    collect(3)
    collect(1)

    stream = 0.1 * xg[0, 0].astype(F32) + own_sum[...] * down_scale_ref[...]
    own_sum[...] = stream
    last_send[...] = jnp.broadcast_to(
        jnp.sum(stream * stream, axis=1, keepdims=True), last_send.shape
    )
    send("last", 0, last_send, last_recv, core_peer)
    arrived("last", 0)
    both = (last_send[...] + last_recv[...])[:, :1]
    rscale = lax.rsqrt(both / features + EPS)
    out_ref[...] = (own_sum[...] * rscale * gain2_ref[...]).astype(BF16)
    for (name, _), copy in copies.items():
        if name[0] != "z":
            copy.wait_send()
    for copy in relays[:2]:
        copy.wait_send()

    @pl.when(inner)
    def _():
        for copy in relays[2:]:
            copy.wait_send()


def fused(
    planes,
    activations,
    gain_first,
    gate_weight,
    gate_scale,
    up_weight,
    up_scale,
    down_weight,
    down_scale,
    gain_second,
):
    rows, width = activations.shape
    units = gate_weight.shape[0]
    half = width // 2
    group = 4 * rows
    n_copies = 24 * planes
    vmem = pl.BlockSpec(memory_space=pltpu.VMEM)
    hbm = pl.BlockSpec(memory_space=pl.ANY)
    scratch = [
        pltpu.VMEM((3, units, width), F32),
        pltpu.VMEM((units, width), BF16),
        pltpu.VMEM((units, width), BF16),
        pltpu.VMEM((units, width), BF16),
        pltpu.VMEM((1, width), F32),
        pltpu.VMEM((units,), F32),
        pltpu.VMEM((units,), F32),
        pltpu.VMEM((1, width), F32),
        pltpu.VMEM((1, width), F32),
        pltpu.VMEM((planes, 4, rows, width), BF16),
        pltpu.VMEM((planes, 4, rows, width), BF16),
        pltpu.VMEM((planes, group, units), BF16),
        pltpu.VMEM((planes, 2, group, units), F32),
        pltpu.VMEM((planes, 2, group, units), BF16),
        pltpu.VMEM((planes, 2, group, units), BF16),
        pltpu.VMEM((planes, 4, rows, 128), F32),
        pltpu.VMEM((planes, 4, rows, 128), F32),
        pltpu.VMEM((planes, 2, rows, half), F32),
        pltpu.VMEM((planes, 2, rows, half), F32),
        pltpu.VMEM((planes, 2, rows, half), BF16),
        pltpu.VMEM((planes, 2, rows, half), BF16),
        pltpu.VMEM((planes, 2, rows, half), BF16),
        pltpu.VMEM((planes, 2, rows, half), BF16),
        pltpu.VMEM((planes, rows, half), BF16),
        pltpu.VMEM((planes, rows, half), BF16),
        pltpu.VMEM((planes, rows, half), BF16),
        pltpu.VMEM((planes, rows, half), BF16),
        pltpu.VMEM((2, rows, half), F32),
        pltpu.VMEM((rows, width), F32),
        pltpu.VMEM((planes, 2, rows, half), BF16),
        pltpu.VMEM((planes, 2, rows, half), BF16),
        pltpu.VMEM((rows, 128), F32),
        pltpu.VMEM((rows, 128), F32),
        pltpu.SemaphoreType.DMA((6,)),
        pltpu.SemaphoreType.DMA((3,)),
        pltpu.SemaphoreType.DMA((n_copies,)),
        pltpu.SemaphoreType.DMA((n_copies,)),
        pltpu.SemaphoreType.DMA((10,)),
        pltpu.SemaphoreType.DMA((planes, 2)),
    ]
    return pl.pallas_call(
        functools.partial(kernel, planes, width * 2),
        out_shape=pltpu.VMEM((rows, width), BF16),
        in_specs=[hbm] * 9,
        out_specs=vmem,
        scratch_shapes=scratch,
        compiler_params=pltpu.CompilerParams(
            collective_id=0, has_side_effects=True, vmem_limit_bytes=60 * 1024 * 1024
        ),
    )(
        activations,
        gain_first[None, :],
        gate_weight,
        gate_scale,
        up_weight,
        up_scale,
        down_weight,
        down_scale[None, :],
        gain_second[None, :],
    )


def plain(
    activations,
    gain_first,
    gate_weight,
    gate_scale,
    up_weight,
    up_scale,
    down_weight,
    down_scale,
    gain_second,
):
    inputs = activations.astype(F32)
    features = activations.shape[1] * lax.axis_size("cb")
    gate_local = gate_weight.astype(BF16)
    up_local = up_weight.astype(BF16)
    down_local = down_weight.astype(BF16)
    gathered = lax.all_gather(activations, "ra", axis=0, tiled=True)
    wide_rows = gathered.astype(F32)
    row_squares = jnp.sum(wide_rows * wide_rows, axis=1)
    scaled = (wide_rows * gain_first).astype(BF16)
    contract = (((1,), (1,)), ((), ()))
    squares = lax.psum(row_squares, "cb")
    gate_part = lax.dot_general(gate_local, scaled, contract, preferred_element_type=F32)
    up_part = lax.dot_general(up_local, scaled, contract, preferred_element_type=F32)
    gate_sum, up_sum = lax.psum((gate_part, up_part), "cb")
    rscale_first = lax.rsqrt(squares / features + EPS)[None, :]
    gate_full = gate_sum * rscale_first * gate_scale[:, None]
    up_full = up_sum * rscale_first * up_scale[:, None]
    hidden = (jax.nn.silu(gate_full) * up_full).astype(BF16)
    mixed = lax.dot_general(hidden, down_local, (((0,), (0,)), ((), ())), preferred_element_type=F32)
    summed = lax.psum_scatter(mixed, "ra", scatter_dimension=0, tiled=True)
    stream = 0.1 * inputs + summed * down_scale
    second = lax.psum(jnp.sum(stream * stream, axis=1), "cb")
    rscale_second = lax.rsqrt(second / features + EPS)[:, None]
    return (stream * rscale_second * gain_second).astype(BF16)


def solution(mesh):
    placed = (
        P("ra", "cb"),
        P("cb"),
        P("ra", "cb"),
        P("ra"),
        P("ra", "cb"),
        P("ra"),
        P("ra", "cb"),
        P("cb"),
        P("cb"),
    )
    planes = mesh.shape["ra"] // 4
    paired = mesh.shape["cb"] == 2 and planes == 4
    body = functools.partial(fused, planes) if paired else plain
    return jax.shard_map(
        body, mesh=mesh, in_specs=placed, out_specs=P("ra", "cb"), check_vma=False
    )
```

```python
import functools

import jax
import jax.numpy as jnp
from jax import lax
from jax.experimental import pallas as pl
from jax.experimental.pallas import tpu as pltpu
from jax.sharding import PartitionSpec as P

EPS = 1e-06
MESH = pl.DeviceIdType.MESH
F32 = jnp.float32
BF16 = jnp.bfloat16


def flip(index, mask):
    bit = 1
    while bit <= mask:
        if mask & bit:
            index = index + (1 - 2 * ((index // bit) % 2)) * bit
        bit *= 2
    return index


def kernel(
    planes,
    features,
    x_hbm,
    gain_hbm,
    gate_hbm,
    gate_scale_hbm,
    up_hbm,
    up_scale_hbm,
    down_hbm,
    down_scale_hbm,
    gain2_hbm,
    out_ref,
    wide,
    gate_w,
    up_w,
    down_w,
    gain_ref,
    gate_scale_ref,
    up_scale_ref,
    down_scale_ref,
    gain2_ref,
    xg,
    scaled,
    hidden,
    part,
    ex_send,
    ex_recv,
    sq_send,
    sq_recv,
    keep_a,
    keep_b,
    send_a,
    send_b,
    recv_a,
    recv_b,
    send2_a,
    send2_b,
    recv2_a,
    recv2_b,
    far,
    own_sum,
    z_send,
    z_recv,
    last_send,
    last_recv,
    in_sem,
    w_sem,
    ssem,
    rsem,
    zs_sem,
    zr_sem,
):
    ra = lax.axis_index("ra")
    cb = lax.axis_index("cb")
    rows, width = xg.shape[2:]
    half = width // 2
    x_peer = (flip(ra, 1), cb)
    y_peer = (flip(ra, 2), cb)
    z_peers = [None] + [(flip(ra, 4 * k), cb) for k in range(1, planes)]
    core_peer = (ra, flip(cb, 1))
    halves = (pl.ds(0, half), pl.ds(half, half))
    first, second = halves

    barrier = pltpu.get_barrier_semaphore()
    peers = [x_peer, y_peer, core_peer] + z_peers[1:]
    for peer in peers:
        pl.semaphore_signal(barrier, inc=1, device_id=peer, device_id_type=MESH)
    own = pltpu.make_async_copy(x_hbm, xg.at[0, 0], in_sem.at[0])
    own.start()
    small = []
    for i, (src, dst) in enumerate(
        (
            (gain_hbm, gain_ref),
            (gate_scale_hbm, gate_scale_ref),
            (up_scale_hbm, up_scale_ref),
            (down_scale_hbm, down_scale_ref),
            (gain2_hbm, gain2_ref),
        )
    ):
        load = pltpu.make_async_copy(src, dst, in_sem.at[i + 1])
        load.start()
        small.append(load)
    loads = []
    for i, src in enumerate((gate_hbm, up_hbm, down_hbm)):
        load = pltpu.make_async_copy(src, wide.at[i], w_sem.at[i])
        load.start()
        loads.append(load)
    own.wait()
    pl.semaphore_wait(barrier, len(peers))

    copies = {}
    slots = []
    landed = {}
    idle = []
    early = list(range(ssem.shape[0]))

    def send(name, k, src, dst, peer):
        slot = len(slots)
        slots.append(name)
        landed[name, k] = rsem.at[slot]
        copy = pltpu.make_async_remote_copy(
            src_ref=src,
            dst_ref=dst,
            send_sem=idle.pop(0) if idle else ssem.at[early.pop(0)],
            recv_sem=rsem.at[slot],
            device_id=peer,
            device_id_type=MESH,
        )
        copy.start()
        copies[name, k] = copy

    seen = set()

    def arrived(name, k):
        if (name, k) in seen:
            return
        seen.add((name, k))
        copies[name, k].wait_recv()
        idle.append(landed[name, k])

    def to_x(k, h):
        send(("gx", h), k, xg.at[k, 0, :, halves[h]], xg.at[k, 1, :, halves[h]], x_peer)

    def to_y(k, h):
        send(("gy", h), k, xg.at[k, 0, :, halves[h]], xg.at[k, 2, :, halves[h]], y_peer)

    level = ra // 4
    inner = level % 2 != level // 2
    relays = []

    def to_z(source, target, h, peer):
        slot = len(relays)
        copy = pltpu.make_async_remote_copy(
            src_ref=xg.at[source, 0, :, halves[h]],
            dst_ref=xg.at[target, 0, :, halves[h]],
            send_sem=zs_sem.at[slot],
            recv_sem=zr_sem.at[target, h],
            device_id=z_peers[peer],
            device_id_type=MESH,
        )
        copies[("z", h), target] = copy
        landed[("z", h), target] = zr_sem.at[target, h]
        relays.append(copy)
        if source or peer != 1:
            pl.when(inner)(copy.start)
        else:
            copy.start()

    def spread(k, h):
        to_x(k, h)
        to_y(k, h)

    def at_z1(h):
        arrived(("z", h), 1)
        to_z(1, 2, h, 3)

    def at_z2(h):
        arrived(("z", h), 2)
        to_z(2, 3, h, 1)
        spread(2, h)

    def relay_z3(h):
        @pl.when(inner)
        def _():
            copies[("z", h), 3].wait_recv()

        to_z(3, 2, h, 1)

    def at_z3(h):
        @pl.when(jnp.logical_not(inner))
        def _():
            copies[("z", h), 3].wait_recv()

        spread(3, h)

    def across(h):
        arrived(("fx", "fy")[h], 0)
        send(("e", h), 1, xg.at[0, 3, :, halves[h]], xg.at[1, 3, :, halves[h]], z_peers[1])

    def forward_y(k):
        arrived(("gx", 1), k)
        send("fy", k, xg.at[k, 1, :, second], xg.at[k, 3, :, second], y_peer)

    def forward_x(k):
        arrived(("gy", 0), k)
        send("fx", k, xg.at[k, 2, :, first], xg.at[k, 3, :, first], x_peer)

    nt = (((1,), (1,)), ((), ()))

    def prepare(k):
        def slot(s):
            block = xg[k, s].astype(F32)
            squares = jnp.sum(block * block, axis=1, keepdims=True)
            sq_send[k, s] = jnp.broadcast_to(squares, (rows, 128))
            scaled[k, s] = (block * gain_ref[...]).astype(BF16)

        slot(0)
        arrived(("gx", 1), k)
        arrived(("gx", 0), k)
        slot(1)
        arrived(("gy", 0), k)
        arrived(("gy", 1), k)
        slot(2)
        if k == 1:
            arrived(("e", 1), 1)
            arrived(("e", 0), 1)
        else:
            arrived("fy", k)
            arrived("fx", k)
        slot(3)
        send("sq", k, sq_send.at[k], sq_recv.at[k], core_peer)

    def product(k, i):
        tokens = scaled[k].reshape(4 * rows, width)
        w = (gate_w, up_w)[i]
        product = lax.dot_general(tokens, w[...], nt, preferred_element_type=F32)
        part[k, i] = product
        ex_send[k, i] = product.astype(BF16)
        send(("ex", i), k, ex_send.at[k, i], ex_recv.at[k, i], core_peer)

    def activate(k):
        arrived("sq", k)
        arrived(("ex", 0), k)
        arrived(("ex", 1), k)
        for s in range(4):
            here = slice(s * rows, (s + 1) * rows)
            squares = (sq_send[k, s] + sq_recv[k, s])[:, :1]
            rscale = lax.rsqrt(squares / features + EPS)
            gate = (part[k, 0, here] + ex_recv[k, 0, here].astype(F32)) * rscale * gate_scale_ref[...][None, :]
            up = (part[k, 1, here] + ex_recv[k, 1, here].astype(F32)) * rscale * up_scale_ref[...][None, :]
            hidden[k, here] = (gate / (1.0 + jnp.exp(-gate)) * up).astype(BF16)

    def down_a(k):
        prod = jnp.dot(hidden[k], down_w[:, :half], preferred_element_type=F32)
        keep_a[k, 0] = prod[:rows]
        send_a[k, 0] = prod[rows : 2 * rows].astype(BF16)
        if k == 1:
            send2_a[k] = prod[2 * rows : 3 * rows].astype(BF16)
        else:
            keep_a[k, 1] = prod[2 * rows : 3 * rows]
        if k:
            send_a[k, 1] = prod[3 * rows :].astype(BF16)
        else:
            far[0] = prod[3 * rows :]

    def down_b(k):
        prod = jnp.dot(hidden[k], down_w[:, half:], preferred_element_type=F32)
        keep_b[k, 0] = prod[:rows]
        send_b[k, 0] = prod[2 * rows : 3 * rows].astype(BF16)
        if k == 1:
            send2_b[k] = prod[rows : 2 * rows].astype(BF16)
        else:
            keep_b[k, 1] = prod[rows : 2 * rows]
        if k:
            send_b[k, 1] = prod[3 * rows :].astype(BF16)
        else:
            far[1] = prod[3 * rows :]

    def one_a(k, d):
        send(("a1", d), k, send_a.at[k, d], recv_a.at[k, d], x_peer)

    def one_b(k, d):
        send(("b1", d), k, send_b.at[k, d], recv_b.at[k, d], y_peer)

    def cross_a():
        send(("r", 0), 1, send_a.at[1, 1], recv_a.at[1, 1], z_peers[1])
        one_a(1, 0)
        send("a2", 1, send2_a.at[1], recv2_a.at[1], y_peer)

    def cross_b():
        send(("r", 1), 1, send_b.at[1, 1], recv_b.at[1, 1], z_peers[1])
        one_b(1, 0)
        send("b2", 1, send2_b.at[1], recv2_b.at[1], x_peer)

    def merge_a():
        arrived(("r", 0), 1)
        send_a[0, 1] = (far[0] + recv_a[1, 1].astype(F32)).astype(BF16)
        one_a(0, 1)

    def merge_b():
        arrived(("r", 1), 1)
        send_b[0, 1] = (far[1] + recv_b[1, 1].astype(F32)).astype(BF16)
        one_b(0, 1)

    def two_a(k):
        arrived(("a1", 1), k)
        send2_a[k] = (keep_a[k, 1] + recv_a[k, 1].astype(F32)).astype(BF16)
        send("a2", k, send2_a.at[k], recv2_a.at[k], y_peer)

    def two_b(k):
        arrived(("b1", 1), k)
        send2_b[k] = (keep_b[k, 1] + recv_b[k, 1].astype(F32)).astype(BF16)
        send("b2", k, send2_b.at[k], recv2_b.at[k], x_peer)

    def home(k, h, mine):
        if k == 0:
            own_sum[:, halves[h]] = mine
            return
        if k == 3:
            arrived(("zs", h), 2)
            mine = mine + z_recv[2, h].astype(F32)
        peer = z_peers[1 if k == 2 else k]
        z_send[k, h] = mine.astype(BF16)
        send(("zs", h), k, z_send.at[k, h], z_recv.at[k, h], peer)

    def home_a(k):
        arrived(("a1", 0), k)
        arrived("a2", k)
        home(k, 0, keep_a[k, 0] + recv_a[k, 0].astype(F32) + recv2_a[k].astype(F32))

    def home_b(k):
        arrived(("b1", 0), k)
        arrived("b2", k)
        home(k, 1, keep_b[k, 0] + recv_b[k, 0].astype(F32) + recv2_b[k].astype(F32))

    def collect(k):
        for h in range(2):
            arrived(("zs", h), k)
            own_sum[:, halves[h]] += z_recv[k, h].astype(F32)

    def narrow(i, target):
        loads[i].wait()
        step = 64

        def body(j, carry):
            here = pl.ds(pl.multiple_of(j * step, step), step)
            target[here] = wide[i, here].astype(BF16)
            return carry

        lax.fori_loop(0, target.shape[0] // step, body, 0)

    for h in (1, 0):
        to_x(0, h)
        to_y(0, 1 - h)
        to_z(0, 1, h, 1)
    for h in (1, 0):
        to_z(0, 3, h, 3)
    narrow(0, gate_w)
    forward_y(0)
    forward_x(0)
    relay_z3(1)
    at_z1(1)
    at_z1(0)
    spread(1, 0)
    relay_z3(0)
    at_z2(1)
    at_z2(0)
    across(1)
    at_z3(1)
    for load in small:
        load.wait()
    prepare(0)
    across(0)
    narrow(1, up_w)
    product(0, 0)
    forward_y(2)
    forward_x(2)
    spread(1, 1)
    product(0, 1)
    narrow(2, down_w)
    activate(0)
    down_a(0)
    one_a(0, 0)
    at_z3(0)
    prepare(2)
    product(2, 0)
    product(2, 1)
    prepare(1)
    forward_y(3)
    forward_x(3)
    product(1, 0)
    activate(2)
    down_b(2)
    down_a(2)
    one_a(2, 1)
    one_b(2, 1)
    one_b(2, 0)
    one_a(2, 0)
    product(1, 1)
    prepare(3)
    product(3, 0)
    product(3, 1)
    two_a(2)
    two_b(2)
    activate(1)
    down_a(1)
    down_b(0)
    cross_a()
    down_b(1)
    activate(3)
    down_a(3)
    down_b(3)
    one_b(3, 1)
    one_a(3, 1)
    cross_b()
    home_b(2)
    two_a(3)
    one_a(3, 0)
    two_b(3)
    one_b(3, 0)
    merge_b()
    merge_a()
    home_a(2)
    home_b(1)
    one_b(0, 0)
    home_a(3)
    home_b(3)
    two_b(0)
    two_a(0)
    home_a(1)
    home_a(0)
    home_b(0)
    collect(3)
    collect(1)

    stream = 0.1 * xg[0, 0].astype(F32) + own_sum[...] * down_scale_ref[...]
    own_sum[...] = stream
    last_send[...] = jnp.broadcast_to(
        jnp.sum(stream * stream, axis=1, keepdims=True), last_send.shape
    )
    send("last", 0, last_send, last_recv, core_peer)
    arrived("last", 0)
    both = (last_send[...] + last_recv[...])[:, :1]
    rscale = lax.rsqrt(both / features + EPS)
    out_ref[...] = (own_sum[...] * rscale * gain2_ref[...]).astype(BF16)
    for (name, _), copy in copies.items():
        if name[0] != "z":
            copy.wait_send()
    for copy in relays[:2]:
        copy.wait_send()

    @pl.when(inner)
    def _():
        for copy in relays[2:]:
            copy.wait_send()


def fused(
    planes,
    activations,
    gain_first,
    gate_weight,
    gate_scale,
    up_weight,
    up_scale,
    down_weight,
    down_scale,
    gain_second,
):
    rows, width = activations.shape
    units = gate_weight.shape[0]
    half = width // 2
    group = 4 * rows
    n_copies = 17 * planes - 1
    vmem = pl.BlockSpec(memory_space=pltpu.VMEM)
    hbm = pl.BlockSpec(memory_space=pl.ANY)
    scratch = [
        pltpu.VMEM((3, units, width), F32),
        pltpu.VMEM((units, width), BF16),
        pltpu.VMEM((units, width), BF16),
        pltpu.VMEM((units, width), BF16),
        pltpu.VMEM((1, width), F32),
        pltpu.VMEM((units,), F32),
        pltpu.VMEM((units,), F32),
        pltpu.VMEM((1, width), F32),
        pltpu.VMEM((1, width), F32),
        pltpu.VMEM((planes, 4, rows, width), BF16),
        pltpu.VMEM((planes, 4, rows, width), BF16),
        pltpu.VMEM((planes, group, units), BF16),
        pltpu.VMEM((planes, 2, group, units), F32),
        pltpu.VMEM((planes, 2, group, units), BF16),
        pltpu.VMEM((planes, 2, group, units), BF16),
        pltpu.VMEM((planes, 4, rows, 128), F32),
        pltpu.VMEM((planes, 4, rows, 128), F32),
        pltpu.VMEM((planes, 2, rows, half), F32),
        pltpu.VMEM((planes, 2, rows, half), F32),
        pltpu.VMEM((planes, 2, rows, half), BF16),
        pltpu.VMEM((planes, 2, rows, half), BF16),
        pltpu.VMEM((planes, 2, rows, half), BF16),
        pltpu.VMEM((planes, 2, rows, half), BF16),
        pltpu.VMEM((planes, rows, half), BF16),
        pltpu.VMEM((planes, rows, half), BF16),
        pltpu.VMEM((planes, rows, half), BF16),
        pltpu.VMEM((planes, rows, half), BF16),
        pltpu.VMEM((2, rows, half), F32),
        pltpu.VMEM((rows, width), F32),
        pltpu.VMEM((planes, 2, rows, half), BF16),
        pltpu.VMEM((planes, 2, rows, half), BF16),
        pltpu.VMEM((rows, 128), F32),
        pltpu.VMEM((rows, 128), F32),
        pltpu.SemaphoreType.DMA((6,)),
        pltpu.SemaphoreType.DMA((3,)),
        pltpu.SemaphoreType.DMA((3 * planes,)),
        pltpu.SemaphoreType.DMA((n_copies,)),
        pltpu.SemaphoreType.DMA((10,)),
        pltpu.SemaphoreType.DMA((planes, 2)),
    ]
    return pl.pallas_call(
        functools.partial(kernel, planes, width * 2),
        out_shape=pltpu.VMEM((rows, width), BF16),
        in_specs=[hbm] * 9,
        out_specs=vmem,
        scratch_shapes=scratch,
        compiler_params=pltpu.CompilerParams(
            collective_id=0, has_side_effects=True, vmem_limit_bytes=60 * 1024 * 1024
        ),
    )(
        activations,
        gain_first[None, :],
        gate_weight,
        gate_scale,
        up_weight,
        up_scale,
        down_weight,
        down_scale[None, :],
        gain_second[None, :],
    )


def plain(
    activations,
    gain_first,
    gate_weight,
    gate_scale,
    up_weight,
    up_scale,
    down_weight,
    down_scale,
    gain_second,
):
    inputs = activations.astype(F32)
    features = activations.shape[1] * lax.axis_size("cb")
    gate_local = gate_weight.astype(BF16)
    up_local = up_weight.astype(BF16)
    down_local = down_weight.astype(BF16)
    gathered = lax.all_gather(activations, "ra", axis=0, tiled=True)
    wide_rows = gathered.astype(F32)
    row_squares = jnp.sum(wide_rows * wide_rows, axis=1)
    scaled = (wide_rows * gain_first).astype(BF16)
    contract = (((1,), (1,)), ((), ()))
    squares = lax.psum(row_squares, "cb")
    gate_part = lax.dot_general(gate_local, scaled, contract, preferred_element_type=F32)
    up_part = lax.dot_general(up_local, scaled, contract, preferred_element_type=F32)
    gate_sum, up_sum = lax.psum((gate_part, up_part), "cb")
    rscale_first = lax.rsqrt(squares / features + EPS)[None, :]
    gate_full = gate_sum * rscale_first * gate_scale[:, None]
    up_full = up_sum * rscale_first * up_scale[:, None]
    hidden = (jax.nn.silu(gate_full) * up_full).astype(BF16)
    mixed = lax.dot_general(hidden, down_local, (((0,), (0,)), ((), ())), preferred_element_type=F32)
    summed = lax.psum_scatter(mixed, "ra", scatter_dimension=0, tiled=True)
    stream = 0.1 * inputs + summed * down_scale
    second = lax.psum(jnp.sum(stream * stream, axis=1), "cb")
    rscale_second = lax.rsqrt(second / features + EPS)[:, None]
    return (stream * rscale_second * gain_second).astype(BF16)


def solution(mesh):
    placed = (
        P("ra", "cb"),
        P("cb"),
        P("ra", "cb"),
        P("ra"),
        P("ra", "cb"),
        P("ra"),
        P("ra", "cb"),
        P("cb"),
        P("cb"),
    )
    planes = mesh.shape["ra"] // 4
    paired = mesh.shape["cb"] == 2 and planes == 4
    body = functools.partial(fused, planes) if paired else plain
    return jax.shard_map(
        body, mesh=mesh, in_specs=placed, out_specs=P("ra", "cb"), check_vma=False
    )
```

```python
import functools

import jax
import jax.numpy as jnp
from jax import lax
from jax.experimental import pallas as pl
from jax.experimental.pallas import tpu as pltpu
from jax.sharding import PartitionSpec as P

EPS = 1e-06
MESH = pl.DeviceIdType.MESH
F32 = jnp.float32
BF16 = jnp.bfloat16


def flip(index, mask):
    bit = 1
    while bit <= mask:
        if mask & bit:
            index = index + (1 - 2 * ((index // bit) % 2)) * bit
        bit *= 2
    return index


def kernel(
    planes,
    features,
    x_hbm,
    gain_hbm,
    gate_hbm,
    gate_scale_hbm,
    up_hbm,
    up_scale_hbm,
    down_hbm,
    down_scale_hbm,
    gain2_hbm,
    out_ref,
    wide,
    gate_w,
    up_w,
    down_w,
    gain_ref,
    gate_scale_ref,
    up_scale_ref,
    down_scale_ref,
    gain2_ref,
    xg,
    scaled,
    hidden,
    part,
    ex_send,
    ex_recv,
    sq_send,
    sq_recv,
    keep_a,
    keep_b,
    send_a,
    send_b,
    recv_a,
    recv_b,
    send2_a,
    send2_b,
    recv2_a,
    recv2_b,
    far,
    own_sum,
    z_send,
    z_recv,
    last_send,
    last_recv,
    in_sem,
    w_sem,
    ssem,
    rsem,
    zs_sem,
    zr_sem,
):
    ra = lax.axis_index("ra")
    cb = lax.axis_index("cb")
    rows, width = xg.shape[2:]
    half = width // 2
    x_peer = (flip(ra, 1), cb)
    y_peer = (flip(ra, 2), cb)
    z_peers = [None] + [(flip(ra, 4 * k), cb) for k in range(1, planes)]
    core_peer = (ra, flip(cb, 1))
    halves = (pl.ds(0, half), pl.ds(half, half))
    first, second = halves

    barrier = pltpu.get_barrier_semaphore()
    peers = [x_peer, y_peer, core_peer] + z_peers[1:]
    for peer in peers:
        pl.semaphore_signal(barrier, inc=1, device_id=peer, device_id_type=MESH)
    own = pltpu.make_async_copy(x_hbm, xg.at[0, 0], in_sem.at[0])
    own.start()
    small = []
    for i, (src, dst) in enumerate(
        (
            (gain_hbm, gain_ref),
            (gate_scale_hbm, gate_scale_ref),
            (up_scale_hbm, up_scale_ref),
            (down_scale_hbm, down_scale_ref),
            (gain2_hbm, gain2_ref),
        )
    ):
        load = pltpu.make_async_copy(src, dst, in_sem.at[i + 1])
        load.start()
        small.append(load)
    loads = []
    for i, src in enumerate((gate_hbm, up_hbm, down_hbm)):
        load = pltpu.make_async_copy(src, wide.at[i], w_sem.at[i])
        load.start()
        loads.append(load)
    own.wait()
    pl.semaphore_wait(barrier, len(peers))

    copies = {}
    slots = []
    landed = {}
    idle = []
    early = list(range(ssem.shape[0]))

    def send(name, k, src, dst, peer):
        slot = len(slots)
        slots.append(name)
        landed[name, k] = rsem.at[slot]
        copy = pltpu.make_async_remote_copy(
            src_ref=src,
            dst_ref=dst,
            send_sem=idle.pop(0) if idle else ssem.at[early.pop(0)],
            recv_sem=rsem.at[slot],
            device_id=peer,
            device_id_type=MESH,
        )
        copy.start()
        copies[name, k] = copy

    seen = set()

    def arrived(name, k):
        if (name, k) in seen:
            return
        seen.add((name, k))
        copies[name, k].wait_recv()
        idle.append(landed[name, k])

    def to_x(k, h):
        send(("gx", h), k, xg.at[k, 0, :, halves[h]], xg.at[k, 1, :, halves[h]], x_peer)

    def to_y(k, h):
        send(("gy", h), k, xg.at[k, 0, :, halves[h]], xg.at[k, 2, :, halves[h]], y_peer)

    level = ra // 4
    inner = level % 2 != level // 2
    relays = []

    def to_z(source, target, h, peer):
        slot = len(relays)
        copy = pltpu.make_async_remote_copy(
            src_ref=xg.at[source, 0, :, halves[h]],
            dst_ref=xg.at[target, 0, :, halves[h]],
            send_sem=zs_sem.at[slot],
            recv_sem=zr_sem.at[target, h],
            device_id=z_peers[peer],
            device_id_type=MESH,
        )
        copies[("z", h), target] = copy
        landed[("z", h), target] = zr_sem.at[target, h]
        relays.append(copy)
        if source or peer != 1:
            pl.when(inner)(copy.start)
        else:
            copy.start()

    def at_z1(h):
        arrived(("z", h), 1)
        to_z(1, 2, h, 3)

    def pass_z2(h):
        arrived(("z", h), 2)
        to_z(2, 3, h, 1)

    def relay_z3(h):
        @pl.when(inner)
        def _():
            copies[("z", h), 3].wait_recv()

        to_z(3, 2, h, 1)

    def wait_z3(h):
        @pl.when(jnp.logical_not(inner))
        def _():
            copies[("z", h), 3].wait_recv()

    def across(h):
        arrived(("fx", "fy")[h], 0)
        send(("e", h), 1, xg.at[0, 3, :, halves[h]], xg.at[1, 3, :, halves[h]], z_peers[1])

    def forward_y(k):
        arrived(("gx", 1), k)
        send("fy", k, xg.at[k, 1, :, second], xg.at[k, 3, :, second], y_peer)

    def forward_x(k):
        arrived(("gy", 0), k)
        send("fx", k, xg.at[k, 2, :, first], xg.at[k, 3, :, first], x_peer)

    nt = (((1,), (1,)), ((), ()))

    def slot(k, s):
        if s == 1:
            arrived(("gx", 1), k)
            arrived(("gx", 0), k)
        elif s == 2:
            arrived(("gy", 0), k)
            arrived(("gy", 1), k)
        elif s == 3:
            for h in (1, 0):
                arrived(("e", h) if k == 1 else ("fx", "fy")[h], k)
        block = xg[k, s].astype(F32)
        total = jnp.sum(block * block, axis=1, keepdims=True)
        sq_send[k, s] = jnp.broadcast_to(total, (rows, 128))
        scaled[k, s] = (block * gain_ref[...]).astype(BF16)

    def squares(k):
        send("sq", k, sq_send.at[k], sq_recv.at[k], core_peer)

    def product(k, i):
        tokens = scaled[k].reshape(4 * rows, width)
        w = (gate_w, up_w)[i]
        product = lax.dot_general(tokens, w[...], nt, preferred_element_type=F32)
        part[k, i] = product
        ex_send[k, i] = product.astype(BF16)
        send(("ex", i), k, ex_send.at[k, i], ex_recv.at[k, i], core_peer)

    def activate(k):
        arrived("sq", k)
        arrived(("ex", 0), k)
        arrived(("ex", 1), k)
        for s in range(4):
            here = slice(s * rows, (s + 1) * rows)
            squares = (sq_send[k, s] + sq_recv[k, s])[:, :1]
            rscale = lax.rsqrt(squares / features + EPS)
            gate = (part[k, 0, here] + ex_recv[k, 0, here].astype(F32)) * rscale * gate_scale_ref[...][None, :]
            up = (part[k, 1, here] + ex_recv[k, 1, here].astype(F32)) * rscale * up_scale_ref[...][None, :]
            hidden[k, here] = (gate / (1.0 + jnp.exp(-gate)) * up).astype(BF16)

    def down_a(k):
        prod = jnp.dot(hidden[k], down_w[:, :half], preferred_element_type=F32)
        keep_a[k, 0] = prod[:rows]
        send_a[k, 0] = prod[rows : 2 * rows].astype(BF16)
        if k == 1:
            send2_a[k] = prod[2 * rows : 3 * rows].astype(BF16)
        else:
            keep_a[k, 1] = prod[2 * rows : 3 * rows]
        if k:
            send_a[k, 1] = prod[3 * rows :].astype(BF16)
        else:
            far[0] = prod[3 * rows :]

    def down_b(k):
        prod = jnp.dot(hidden[k], down_w[:, half:], preferred_element_type=F32)
        keep_b[k, 0] = prod[:rows]
        send_b[k, 0] = prod[2 * rows : 3 * rows].astype(BF16)
        if k == 1:
            send2_b[k] = prod[rows : 2 * rows].astype(BF16)
        else:
            keep_b[k, 1] = prod[rows : 2 * rows]
        if k:
            send_b[k, 1] = prod[3 * rows :].astype(BF16)
        else:
            far[1] = prod[3 * rows :]

    def one_a(k, d):
        send(("a1", d), k, send_a.at[k, d], recv_a.at[k, d], x_peer)

    def one_b(k, d):
        send(("b1", d), k, send_b.at[k, d], recv_b.at[k, d], y_peer)

    def send_r(h):
        src, dst = ((send_a, recv_a), (send_b, recv_b))[h]
        send(("r", h), 1, src.at[1, 1], dst.at[1, 1], z_peers[1])

    def pass_a():
        send("a2", 1, send2_a.at[1], recv2_a.at[1], y_peer)

    def pass_b():
        send("b2", 1, send2_b.at[1], recv2_b.at[1], x_peer)

    def merge_a():
        arrived(("r", 0), 1)
        send_a[0, 1] = (far[0] + recv_a[1, 1].astype(F32)).astype(BF16)
        one_a(0, 1)

    def merge_b():
        arrived(("r", 1), 1)
        send_b[0, 1] = (far[1] + recv_b[1, 1].astype(F32)).astype(BF16)
        one_b(0, 1)

    def two_a(k):
        arrived(("a1", 1), k)
        send2_a[k] = (keep_a[k, 1] + recv_a[k, 1].astype(F32)).astype(BF16)
        send("a2", k, send2_a.at[k], recv2_a.at[k], y_peer)

    def two_b(k):
        arrived(("b1", 1), k)
        send2_b[k] = (keep_b[k, 1] + recv_b[k, 1].astype(F32)).astype(BF16)
        send("b2", k, send2_b.at[k], recv2_b.at[k], x_peer)

    def home(k, h, mine):
        if k == 0:
            own_sum[:, halves[h]] = mine
            return
        if k == 3:
            arrived(("zs", h), 2)
            mine = mine + z_recv[2, h].astype(F32)
        peer = z_peers[1 if k == 2 else k]
        z_send[k, h] = mine.astype(BF16)
        send(("zs", h), k, z_send.at[k, h], z_recv.at[k, h], peer)

    def home_a(k):
        arrived(("a1", 0), k)
        arrived("a2", k)
        home(k, 0, keep_a[k, 0] + recv_a[k, 0].astype(F32) + recv2_a[k].astype(F32))

    def home_b(k):
        arrived(("b1", 0), k)
        arrived("b2", k)
        home(k, 1, keep_b[k, 0] + recv_b[k, 0].astype(F32) + recv2_b[k].astype(F32))

    def collect(k):
        for h in range(2):
            arrived(("zs", h), k)
            own_sum[:, halves[h]] += z_recv[k, h].astype(F32)

    def narrow(i, target):
        loads[i].wait()
        step = 64

        def body(j, carry):
            here = pl.ds(pl.multiple_of(j * step, step), step)
            target[here] = wide[i, here].astype(BF16)
            return carry

        lax.fori_loop(0, target.shape[0] // step, body, 0)

    for h in (1, 0):
        to_x(0, h)
        to_y(0, 1 - h)
        to_z(0, 1, h, 1)
    for h in (1, 0):
        to_z(0, 3, h, 3)
    relay_z3(1)
    at_z1(1)
    to_y(1, 1)
    forward_x(0)
    to_x(1, 1)
    at_z1(0)
    forward_y(0)
    relay_z3(0)
    for load in small:
        load.wait()
    slot(0, 2)
    narrow(0, gate_w)
    pass_z2(1)
    to_x(2, 1)
    to_y(1, 0)
    narrow(1, up_w)
    to_x(1, 0)
    narrow(2, down_w)
    slot(0, 0)
    pass_z2(0)
    slot(0, 3)
    to_y(2, 0)
    slot(0, 1)
    across(1)
    across(0)
    product(0, 0)
    wait_z3(1)
    to_y(2, 1)
    to_x(3, 1)
    slot(1, 0)
    slot(1, 2)
    forward_y(2)
    to_x(2, 0)
    forward_x(2)
    slot(1, 1)
    wait_z3(0)
    to_y(3, 0)
    slot(2, 0)
    product(0, 1)
    slot(1, 3)
    product(1, 1)
    slot(2, 1)
    squares(1)
    squares(0)
    product(1, 0)
    slot(2, 2)
    to_y(3, 1)
    to_x(3, 0)
    forward_x(3)
    slot(2, 3)
    forward_y(3)
    product(2, 0)
    squares(2)
    product(2, 1)
    activate(1)
    down_a(1)
    one_a(1, 0)
    down_b(1)
    pass_a()
    activate(2)
    down_b(2)
    one_b(2, 1)
    pass_b()
    slot(3, 1)
    down_a(2)
    slot(3, 0)
    activate(0)
    one_a(2, 1)
    send_r(1)
    down_a(0)
    slot(3, 2)
    one_b(1, 0)
    slot(3, 3)
    one_a(2, 0)
    one_b(2, 0)
    squares(3)
    send_r(0)
    product(3, 0)
    product(3, 1)
    home_a(1)
    two_b(2)
    activate(3)
    down_b(3)
    one_b(3, 1)
    home_b(1)
    two_a(2)
    down_b(0)
    down_a(3)
    one_a(3, 1)
    home_b(2)
    two_b(3)
    one_b(3, 0)
    one_a(3, 0)
    two_a(3)
    merge_b()
    one_b(0, 0)
    merge_a()
    home_a(2)
    one_a(0, 0)
    home_b(3)
    home_a(3)
    two_b(0)
    two_a(0)
    home_b(0)
    home_a(0)
    collect(1)
    collect(3)

    stream = 0.1 * xg[0, 0].astype(F32) + own_sum[...] * down_scale_ref[...]
    own_sum[...] = stream
    last_send[...] = jnp.broadcast_to(
        jnp.sum(stream * stream, axis=1, keepdims=True), last_send.shape
    )
    send("last", 0, last_send, last_recv, core_peer)
    arrived("last", 0)
    both = (last_send[...] + last_recv[...])[:, :1]
    rscale = lax.rsqrt(both / features + EPS)
    out_ref[...] = (own_sum[...] * rscale * gain2_ref[...]).astype(BF16)
    for (name, _), copy in copies.items():
        if name[0] != "z":
            copy.wait_send()
    for copy in relays[:2]:
        copy.wait_send()

    @pl.when(inner)
    def _():
        for copy in relays[2:]:
            copy.wait_send()


def fused(
    planes,
    activations,
    gain_first,
    gate_weight,
    gate_scale,
    up_weight,
    up_scale,
    down_weight,
    down_scale,
    gain_second,
):
    rows, width = activations.shape
    units = gate_weight.shape[0]
    half = width // 2
    group = 4 * rows
    n_copies = 17 * planes - 1
    vmem = pl.BlockSpec(memory_space=pltpu.VMEM)
    hbm = pl.BlockSpec(memory_space=pl.ANY)
    scratch = [
        pltpu.VMEM((3, units, width), F32),
        pltpu.VMEM((units, width), BF16),
        pltpu.VMEM((units, width), BF16),
        pltpu.VMEM((units, width), BF16),
        pltpu.VMEM((1, width), F32),
        pltpu.VMEM((units,), F32),
        pltpu.VMEM((units,), F32),
        pltpu.VMEM((1, width), F32),
        pltpu.VMEM((1, width), F32),
        pltpu.VMEM((planes, 4, rows, width), BF16),
        pltpu.VMEM((planes, 4, rows, width), BF16),
        pltpu.VMEM((planes, group, units), BF16),
        pltpu.VMEM((planes, 2, group, units), F32),
        pltpu.VMEM((planes, 2, group, units), BF16),
        pltpu.VMEM((planes, 2, group, units), BF16),
        pltpu.VMEM((planes, 4, rows, 128), F32),
        pltpu.VMEM((planes, 4, rows, 128), F32),
        pltpu.VMEM((planes, 2, rows, half), F32),
        pltpu.VMEM((planes, 2, rows, half), F32),
        pltpu.VMEM((planes, 2, rows, half), BF16),
        pltpu.VMEM((planes, 2, rows, half), BF16),
        pltpu.VMEM((planes, 2, rows, half), BF16),
        pltpu.VMEM((planes, 2, rows, half), BF16),
        pltpu.VMEM((planes, rows, half), BF16),
        pltpu.VMEM((planes, rows, half), BF16),
        pltpu.VMEM((planes, rows, half), BF16),
        pltpu.VMEM((planes, rows, half), BF16),
        pltpu.VMEM((2, rows, half), F32),
        pltpu.VMEM((rows, width), F32),
        pltpu.VMEM((planes, 2, rows, half), BF16),
        pltpu.VMEM((planes, 2, rows, half), BF16),
        pltpu.VMEM((rows, 128), F32),
        pltpu.VMEM((rows, 128), F32),
        pltpu.SemaphoreType.DMA((6,)),
        pltpu.SemaphoreType.DMA((3,)),
        pltpu.SemaphoreType.DMA((3 * planes,)),
        pltpu.SemaphoreType.DMA((n_copies,)),
        pltpu.SemaphoreType.DMA((10,)),
        pltpu.SemaphoreType.DMA((planes, 2)),
    ]
    return pl.pallas_call(
        functools.partial(kernel, planes, width * 2),
        out_shape=pltpu.VMEM((rows, width), BF16),
        in_specs=[hbm] * 9,
        out_specs=vmem,
        scratch_shapes=scratch,
        compiler_params=pltpu.CompilerParams(
            collective_id=0, has_side_effects=True, vmem_limit_bytes=60 * 1024 * 1024
        ),
    )(
        activations,
        gain_first[None, :],
        gate_weight,
        gate_scale,
        up_weight,
        up_scale,
        down_weight,
        down_scale[None, :],
        gain_second[None, :],
    )


def plain(
    activations,
    gain_first,
    gate_weight,
    gate_scale,
    up_weight,
    up_scale,
    down_weight,
    down_scale,
    gain_second,
):
    inputs = activations.astype(F32)
    features = activations.shape[1] * lax.axis_size("cb")
    gate_local = gate_weight.astype(BF16)
    up_local = up_weight.astype(BF16)
    down_local = down_weight.astype(BF16)
    gathered = lax.all_gather(activations, "ra", axis=0, tiled=True)
    wide_rows = gathered.astype(F32)
    row_squares = jnp.sum(wide_rows * wide_rows, axis=1)
    scaled = (wide_rows * gain_first).astype(BF16)
    contract = (((1,), (1,)), ((), ()))
    squares = lax.psum(row_squares, "cb")
    gate_part = lax.dot_general(gate_local, scaled, contract, preferred_element_type=F32)
    up_part = lax.dot_general(up_local, scaled, contract, preferred_element_type=F32)
    gate_sum, up_sum = lax.psum((gate_part, up_part), "cb")
    rscale_first = lax.rsqrt(squares / features + EPS)[None, :]
    gate_full = gate_sum * rscale_first * gate_scale[:, None]
    up_full = up_sum * rscale_first * up_scale[:, None]
    hidden = (jax.nn.silu(gate_full) * up_full).astype(BF16)
    mixed = lax.dot_general(hidden, down_local, (((0,), (0,)), ((), ())), preferred_element_type=F32)
    summed = lax.psum_scatter(mixed, "ra", scatter_dimension=0, tiled=True)
    stream = 0.1 * inputs + summed * down_scale
    second = lax.psum(jnp.sum(stream * stream, axis=1), "cb")
    rscale_second = lax.rsqrt(second / features + EPS)[:, None]
    return (stream * rscale_second * gain_second).astype(BF16)


def solution(mesh):
    placed = (
        P("ra", "cb"),
        P("cb"),
        P("ra", "cb"),
        P("ra"),
        P("ra", "cb"),
        P("ra"),
        P("ra", "cb"),
        P("cb"),
        P("cb"),
    )
    planes = mesh.shape["ra"] // 4
    paired = mesh.shape["cb"] == 2 and planes == 4
    body = functools.partial(fused, planes) if paired else plain
    return jax.shard_map(
        body, mesh=mesh, in_specs=placed, out_specs=P("ra", "cb"), check_vma=False
    )
```

```python
import functools

import jax
import jax.numpy as jnp
from jax import lax
from jax.experimental import pallas as pl
from jax.experimental.pallas import tpu as pltpu
from jax.sharding import PartitionSpec as P

EPS = 1e-06
MESH = pl.DeviceIdType.MESH
F32 = jnp.float32
BF16 = jnp.bfloat16


def flip(index, mask):
    bit = 1
    while bit <= mask:
        if mask & bit:
            index = index + (1 - 2 * ((index // bit) % 2)) * bit
        bit *= 2
    return index


def kernel(
    planes,
    features,
    x_hbm,
    gain_hbm,
    gate_hbm,
    gate_scale_hbm,
    up_hbm,
    up_scale_hbm,
    down_hbm,
    down_scale_hbm,
    gain2_hbm,
    out_ref,
    wide,
    gate_w,
    up_w,
    down_w,
    gain_ref,
    gate_scale_ref,
    up_scale_ref,
    down_scale_ref,
    gain2_ref,
    xg,
    scaled,
    hidden,
    part,
    ex_send,
    ex_recv,
    sq_send,
    sq_recv,
    keep_a,
    keep_b,
    send_a,
    send_b,
    recv_a,
    recv_b,
    send2_a,
    send2_b,
    recv2_a,
    recv2_b,
    far,
    own_sum,
    z_send,
    z_recv,
    last_send,
    last_recv,
    in_sem,
    w_sem,
    ssem,
    rsem,
    zs_sem,
    zr_sem,
):
    ra = lax.axis_index("ra")
    cb = lax.axis_index("cb")
    rows, width = xg.shape[2:]
    half = width // 2
    x_peer = (flip(ra, 1), cb)
    y_peer = (flip(ra, 2), cb)
    z_peers = [None] + [(flip(ra, 4 * k), cb) for k in range(1, planes)]
    core_peer = (ra, flip(cb, 1))
    halves = (pl.ds(0, half), pl.ds(half, half))
    first, second = halves

    barrier = pltpu.get_barrier_semaphore()
    peers = [x_peer, y_peer, core_peer] + z_peers[1:]
    for peer in peers:
        pl.semaphore_signal(barrier, inc=1, device_id=peer, device_id_type=MESH)
    own = pltpu.make_async_copy(x_hbm, xg.at[0, 0], in_sem.at[0])
    own.start()
    small = []
    for i, (src, dst) in enumerate(
        (
            (gain_hbm, gain_ref),
            (gate_scale_hbm, gate_scale_ref),
            (up_scale_hbm, up_scale_ref),
            (down_scale_hbm, down_scale_ref),
            (gain2_hbm, gain2_ref),
        )
    ):
        load = pltpu.make_async_copy(src, dst, in_sem.at[i + 1])
        load.start()
        small.append(load)
    loads = []
    for i, src in enumerate((gate_hbm, up_hbm, down_hbm)):
        load = pltpu.make_async_copy(src, wide.at[i], w_sem.at[i])
        load.start()
        loads.append(load)
    own.wait()
    pl.semaphore_wait(barrier, len(peers))

    copies = {}
    slots = []
    landed = {}
    idle = []
    early = list(range(ssem.shape[0]))

    def send(name, k, src, dst, peer):
        slot = len(slots)
        slots.append(name)
        landed[name, k] = rsem.at[slot]
        copy = pltpu.make_async_remote_copy(
            src_ref=src,
            dst_ref=dst,
            send_sem=idle.pop(0) if idle else ssem.at[early.pop(0)],
            recv_sem=rsem.at[slot],
            device_id=peer,
            device_id_type=MESH,
        )
        copy.start()
        copies[name, k] = copy

    seen = set()

    def arrived(name, k):
        if (name, k) in seen:
            return
        seen.add((name, k))
        copies[name, k].wait_recv()
        idle.append(landed[name, k])

    def to_x(k, h):
        send(("gx", h), k, xg.at[k, 0, :, halves[h]], xg.at[k, 1, :, halves[h]], x_peer)

    def to_y(k, h):
        send(("gy", h), k, xg.at[k, 0, :, halves[h]], xg.at[k, 2, :, halves[h]], y_peer)

    level = ra // 4
    inner = level % 2 != level // 2
    relays = []

    def to_z(source, target, h, peer):
        slot = len(relays)
        copy = pltpu.make_async_remote_copy(
            src_ref=xg.at[source, 0, :, halves[h]],
            dst_ref=xg.at[target, 0, :, halves[h]],
            send_sem=zs_sem.at[slot],
            recv_sem=zr_sem.at[target, h],
            device_id=z_peers[peer],
            device_id_type=MESH,
        )
        copies[("z", h), target] = copy
        landed[("z", h), target] = zr_sem.at[target, h]
        relays.append(copy)
        if source or peer != 1:
            pl.when(inner)(copy.start)
        else:
            copy.start()

    def at_z1(h):
        arrived(("z", h), 1)
        to_z(1, 2, h, 3)

    def pass_z2(h):
        arrived(("z", h), 2)
        to_z(2, 3, h, 1)

    def relay_z3(h):
        @pl.when(inner)
        def _():
            copies[("z", h), 3].wait_recv()

        to_z(3, 2, h, 1)

    def wait_z3(h):
        @pl.when(jnp.logical_not(inner))
        def _():
            copies[("z", h), 3].wait_recv()

    def across(h):
        arrived(("fx", "fy")[h], 0)
        send(("e", h), 1, xg.at[0, 3, :, halves[h]], xg.at[1, 3, :, halves[h]], z_peers[1])

    def forward_y(k):
        arrived(("gx", 1), k)
        send("fy", k, xg.at[k, 1, :, second], xg.at[k, 3, :, second], y_peer)

    def forward_x(k):
        arrived(("gy", 0), k)
        send("fx", k, xg.at[k, 2, :, first], xg.at[k, 3, :, first], x_peer)

    nt = (((1,), (1,)), ((), ()))

    def slot(k, s):
        if s == 1:
            arrived(("gx", 1), k)
            arrived(("gx", 0), k)
        elif s == 2:
            arrived(("gy", 0), k)
            arrived(("gy", 1), k)
        elif s == 3:
            for h in (1, 0):
                arrived(("e", h) if k == 1 else ("fx", "fy")[h], k)
        block = xg[k, s].astype(F32)
        total = jnp.sum(block * block, axis=1, keepdims=True)
        sq_send[k, s] = jnp.broadcast_to(total, (rows, 128))
        scaled[k, s] = (block * gain_ref[...]).astype(BF16)

    def squares(k):
        send("sq", k, sq_send.at[k], sq_recv.at[k], core_peer)

    def product(k, i):
        tokens = scaled[k].reshape(4 * rows, width)
        w = (gate_w, up_w)[i]
        product = lax.dot_general(tokens, w[...], nt, preferred_element_type=F32)
        part[k, i] = product
        ex_send[k, i] = product.astype(BF16)
        send(("ex", i), k, ex_send.at[k, i], ex_recv.at[k, i], core_peer)

    def activate(k):
        arrived("sq", k)
        arrived(("ex", 0), k)
        arrived(("ex", 1), k)
        for s in range(4):
            here = slice(s * rows, (s + 1) * rows)
            squares = (sq_send[k, s] + sq_recv[k, s])[:, :1]
            rscale = lax.rsqrt(squares / features + EPS)
            gate = (part[k, 0, here] + ex_recv[k, 0, here].astype(F32)) * rscale * gate_scale_ref[...][None, :]
            up = (part[k, 1, here] + ex_recv[k, 1, here].astype(F32)) * rscale * up_scale_ref[...][None, :]
            hidden[k, here] = (gate / (1.0 + jnp.exp(-gate)) * up).astype(BF16)

    def down_a(k):
        prod = jnp.dot(hidden[k], down_w[:, :half], preferred_element_type=F32)
        keep_a[k, 0] = prod[:rows]
        send_a[k, 0] = prod[rows : 2 * rows].astype(BF16)
        if k == 1:
            send2_a[k] = prod[2 * rows : 3 * rows].astype(BF16)
        else:
            keep_a[k, 1] = prod[2 * rows : 3 * rows]
        if k:
            send_a[k, 1] = prod[3 * rows :].astype(BF16)
        else:
            far[0] = prod[3 * rows :]

    def down_b(k):
        prod = jnp.dot(hidden[k], down_w[:, half:], preferred_element_type=F32)
        keep_b[k, 0] = prod[:rows]
        send_b[k, 0] = prod[2 * rows : 3 * rows].astype(BF16)
        if k == 1:
            send2_b[k] = prod[rows : 2 * rows].astype(BF16)
        else:
            keep_b[k, 1] = prod[rows : 2 * rows]
        if k:
            send_b[k, 1] = prod[3 * rows :].astype(BF16)
        else:
            far[1] = prod[3 * rows :]

    def one_a(k, d):
        send(("a1", d), k, send_a.at[k, d], recv_a.at[k, d], x_peer)

    def one_b(k, d):
        send(("b1", d), k, send_b.at[k, d], recv_b.at[k, d], y_peer)

    def send_r(h):
        src, dst = ((send_a, recv_a), (send_b, recv_b))[h]
        send(("r", h), 1, src.at[1, 1], dst.at[1, 1], z_peers[1])

    def pass_a():
        send("a2", 1, send2_a.at[1], recv2_a.at[1], y_peer)

    def pass_b():
        send("b2", 1, send2_b.at[1], recv2_b.at[1], x_peer)

    def merge_a():
        arrived(("r", 0), 1)
        send_a[0, 1] = (far[0] + recv_a[1, 1].astype(F32)).astype(BF16)
        one_a(0, 1)

    def merge_b():
        arrived(("r", 1), 1)
        send_b[0, 1] = (far[1] + recv_b[1, 1].astype(F32)).astype(BF16)
        one_b(0, 1)

    def two_a(k):
        arrived(("a1", 1), k)
        send2_a[k] = (keep_a[k, 1] + recv_a[k, 1].astype(F32)).astype(BF16)
        send("a2", k, send2_a.at[k], recv2_a.at[k], y_peer)

    def two_b(k):
        arrived(("b1", 1), k)
        send2_b[k] = (keep_b[k, 1] + recv_b[k, 1].astype(F32)).astype(BF16)
        send("b2", k, send2_b.at[k], recv2_b.at[k], x_peer)

    def home(k, h, mine):
        if k == 0:
            own_sum[:, halves[h]] = mine
            return
        if k == 3:
            arrived(("zs", h), 2)
            mine = mine + z_recv[2, h].astype(F32)
        peer = z_peers[1 if k == 2 else k]
        z_send[k, h] = mine.astype(BF16)
        send(("zs", h), k, z_send.at[k, h], z_recv.at[k, h], peer)

    def home_a(k):
        arrived(("a1", 0), k)
        arrived("a2", k)
        home(k, 0, keep_a[k, 0] + recv_a[k, 0].astype(F32) + recv2_a[k].astype(F32))

    def home_b(k):
        arrived(("b1", 0), k)
        arrived("b2", k)
        home(k, 1, keep_b[k, 0] + recv_b[k, 0].astype(F32) + recv2_b[k].astype(F32))

    def collect(k):
        for h in range(2):
            arrived(("zs", h), k)
            own_sum[:, halves[h]] += z_recv[k, h].astype(F32)

    def narrow(i, target):
        loads[i].wait()
        step = 64

        def body(j, carry):
            here = pl.ds(pl.multiple_of(j * step, step), step)
            target[here] = wide[i, here].astype(BF16)
            return carry

        lax.fori_loop(0, target.shape[0] // step, body, 0)

    for h in (1, 0):
        to_x(0, h)
        to_y(0, 1 - h)
        to_z(0, 1, h, 1)
    for h in (1, 0):
        to_z(0, 3, h, 3)
    relay_z3(1)
    at_z1(1)
    forward_y(0)
    forward_x(0)
    at_z1(0)
    relay_z3(0)
    to_y(1, 0)
    to_x(1, 1)
    to_y(1, 1)
    for load in small:
        load.wait()
    slot(1, 0)
    pass_z2(1)
    to_x(2, 1)
    slot(0, 3)
    pass_z2(0)
    to_y(2, 0)
    to_x(1, 0)
    slot(0, 0)
    slot(0, 1)
    to_y(2, 1)
    to_x(2, 0)
    slot(0, 2)
    narrow(0, gate_w)
    across(0)
    across(1)
    forward_y(2)
    wait_z3(1)
    product(0, 0)
    to_x(3, 1)
    narrow(2, down_w)
    narrow(1, up_w)
    forward_x(2)
    wait_z3(0)
    slot(1, 2)
    to_y(3, 0)
    squares(0)
    product(0, 1)
    slot(1, 1)
    slot(2, 0)
    slot(2, 2)
    slot(2, 1)
    slot(1, 3)
    product(1, 0)
    product(1, 1)
    forward_x(3)
    to_y(3, 1)
    squares(1)
    slot(2, 3)
    forward_y(3)
    squares(2)
    to_x(3, 0)
    product(2, 0)
    product(2, 1)
    activate(1)
    down_a(1)
    slot(3, 0)
    one_a(1, 0)
    pass_a()
    down_b(1)
    activate(0)
    pass_b()
    activate(2)
    down_a(2)
    one_a(2, 0)
    one_b(1, 0)
    send_r(0)
    down_b(2)
    one_a(2, 1)
    send_r(1)
    slot(3, 2)
    slot(3, 1)
    slot(3, 3)
    one_b(2, 1)
    one_b(2, 0)
    squares(3)
    product(3, 0)
    product(3, 1)
    down_b(0)
    down_a(0)
    activate(3)
    down_b(3)
    one_b(3, 1)
    two_b(2)
    home_a(1)
    down_a(3)
    one_a(3, 1)
    two_a(2)
    home_b(1)
    one_b(3, 0)
    two_b(3)
    one_a(3, 0)
    home_b(2)
    two_a(3)
    home_a(2)
    merge_b()
    one_b(0, 0)
    merge_a()
    one_a(0, 0)
    home_b(3)
    home_a(3)
    two_b(0)
    two_a(0)
    home_a(0)
    home_b(0)
    collect(1)
    collect(3)

    stream = 0.1 * xg[0, 0].astype(F32) + own_sum[...] * down_scale_ref[...]
    own_sum[...] = stream
    last_send[...] = jnp.broadcast_to(
        jnp.sum(stream * stream, axis=1, keepdims=True), last_send.shape
    )
    send("last", 0, last_send, last_recv, core_peer)
    arrived("last", 0)
    both = (last_send[...] + last_recv[...])[:, :1]
    rscale = lax.rsqrt(both / features + EPS)
    out_ref[...] = (own_sum[...] * rscale * gain2_ref[...]).astype(BF16)
    for (name, _), copy in copies.items():
        if name[0] != "z":
            copy.wait_send()
    for copy in relays[:2]:
        copy.wait_send()

    @pl.when(inner)
    def _():
        for copy in relays[2:]:
            copy.wait_send()


def fused(
    planes,
    activations,
    gain_first,
    gate_weight,
    gate_scale,
    up_weight,
    up_scale,
    down_weight,
    down_scale,
    gain_second,
):
    rows, width = activations.shape
    units = gate_weight.shape[0]
    half = width // 2
    group = 4 * rows
    n_copies = 17 * planes - 1
    vmem = pl.BlockSpec(memory_space=pltpu.VMEM)
    hbm = pl.BlockSpec(memory_space=pl.ANY)
    scratch = [
        pltpu.VMEM((3, units, width), F32),
        pltpu.VMEM((units, width), BF16),
        pltpu.VMEM((units, width), BF16),
        pltpu.VMEM((units, width), BF16),
        pltpu.VMEM((1, width), F32),
        pltpu.VMEM((units,), F32),
        pltpu.VMEM((units,), F32),
        pltpu.VMEM((1, width), F32),
        pltpu.VMEM((1, width), F32),
        pltpu.VMEM((planes, 4, rows, width), BF16),
        pltpu.VMEM((planes, 4, rows, width), BF16),
        pltpu.VMEM((planes, group, units), BF16),
        pltpu.VMEM((planes, 2, group, units), F32),
        pltpu.VMEM((planes, 2, group, units), BF16),
        pltpu.VMEM((planes, 2, group, units), BF16),
        pltpu.VMEM((planes, 4, rows, 128), F32),
        pltpu.VMEM((planes, 4, rows, 128), F32),
        pltpu.VMEM((planes, 2, rows, half), F32),
        pltpu.VMEM((planes, 2, rows, half), F32),
        pltpu.VMEM((planes, 2, rows, half), BF16),
        pltpu.VMEM((planes, 2, rows, half), BF16),
        pltpu.VMEM((planes, 2, rows, half), BF16),
        pltpu.VMEM((planes, 2, rows, half), BF16),
        pltpu.VMEM((planes, rows, half), BF16),
        pltpu.VMEM((planes, rows, half), BF16),
        pltpu.VMEM((planes, rows, half), BF16),
        pltpu.VMEM((planes, rows, half), BF16),
        pltpu.VMEM((2, rows, half), F32),
        pltpu.VMEM((rows, width), F32),
        pltpu.VMEM((planes, 2, rows, half), BF16),
        pltpu.VMEM((planes, 2, rows, half), BF16),
        pltpu.VMEM((rows, 128), F32),
        pltpu.VMEM((rows, 128), F32),
        pltpu.SemaphoreType.DMA((6,)),
        pltpu.SemaphoreType.DMA((3,)),
        pltpu.SemaphoreType.DMA((3 * planes,)),
        pltpu.SemaphoreType.DMA((n_copies,)),
        pltpu.SemaphoreType.DMA((10,)),
        pltpu.SemaphoreType.DMA((planes, 2)),
    ]
    return pl.pallas_call(
        functools.partial(kernel, planes, width * 2),
        out_shape=pltpu.VMEM((rows, width), BF16),
        in_specs=[hbm] * 9,
        out_specs=vmem,
        scratch_shapes=scratch,
        compiler_params=pltpu.CompilerParams(
            collective_id=0, has_side_effects=True, vmem_limit_bytes=60 * 1024 * 1024
        ),
    )(
        activations,
        gain_first[None, :],
        gate_weight,
        gate_scale,
        up_weight,
        up_scale,
        down_weight,
        down_scale[None, :],
        gain_second[None, :],
    )


def plain(
    activations,
    gain_first,
    gate_weight,
    gate_scale,
    up_weight,
    up_scale,
    down_weight,
    down_scale,
    gain_second,
):
    inputs = activations.astype(F32)
    features = activations.shape[1] * lax.axis_size("cb")
    gate_local = gate_weight.astype(BF16)
    up_local = up_weight.astype(BF16)
    down_local = down_weight.astype(BF16)
    gathered = lax.all_gather(activations, "ra", axis=0, tiled=True)
    wide_rows = gathered.astype(F32)
    row_squares = jnp.sum(wide_rows * wide_rows, axis=1)
    scaled = (wide_rows * gain_first).astype(BF16)
    contract = (((1,), (1,)), ((), ()))
    squares = lax.psum(row_squares, "cb")
    gate_part = lax.dot_general(gate_local, scaled, contract, preferred_element_type=F32)
    up_part = lax.dot_general(up_local, scaled, contract, preferred_element_type=F32)
    gate_sum, up_sum = lax.psum((gate_part, up_part), "cb")
    rscale_first = lax.rsqrt(squares / features + EPS)[None, :]
    gate_full = gate_sum * rscale_first * gate_scale[:, None]
    up_full = up_sum * rscale_first * up_scale[:, None]
    hidden = (jax.nn.silu(gate_full) * up_full).astype(BF16)
    mixed = lax.dot_general(hidden, down_local, (((0,), (0,)), ((), ())), preferred_element_type=F32)
    summed = lax.psum_scatter(mixed, "ra", scatter_dimension=0, tiled=True)
    stream = 0.1 * inputs + summed * down_scale
    second = lax.psum(jnp.sum(stream * stream, axis=1), "cb")
    rscale_second = lax.rsqrt(second / features + EPS)[:, None]
    return (stream * rscale_second * gain_second).astype(BF16)


def solution(mesh):
    placed = (
        P("ra", "cb"),
        P("cb"),
        P("ra", "cb"),
        P("ra"),
        P("ra", "cb"),
        P("ra"),
        P("ra", "cb"),
        P("cb"),
        P("cb"),
    )
    planes = mesh.shape["ra"] // 4
    paired = mesh.shape["cb"] == 2 and planes == 4
    body = functools.partial(fused, planes) if paired else plain
    return jax.shard_map(
        body, mesh=mesh, in_specs=placed, out_specs=P("ra", "cb"), check_vma=False
    )
```

```python
import functools

import jax
import jax.numpy as jnp
from jax import lax
from jax.experimental import pallas as pl
from jax.experimental.pallas import tpu as pltpu
from jax.sharding import PartitionSpec as P

EPS = 1e-06
MESH = pl.DeviceIdType.MESH
F32 = jnp.float32
BF16 = jnp.bfloat16


def flip(index, mask):
    bit = 1
    while bit <= mask:
        if mask & bit:
            index = index + (1 - 2 * ((index // bit) % 2)) * bit
        bit *= 2
    return index


def kernel(
    planes,
    features,
    x_hbm,
    gain_hbm,
    gate_hbm,
    gate_scale_hbm,
    up_hbm,
    up_scale_hbm,
    down_hbm,
    down_scale_hbm,
    gain2_hbm,
    out_ref,
    wide,
    gate_w,
    up_w,
    down_w,
    gain_ref,
    gate_scale_ref,
    up_scale_ref,
    down_scale_ref,
    gain2_ref,
    xg,
    scaled,
    hidden,
    part,
    ex_send,
    ex_recv,
    sq_send,
    sq_recv,
    keep_a,
    keep_b,
    send_a,
    send_b,
    recv_a,
    recv_b,
    send2_a,
    send2_b,
    recv2_a,
    recv2_b,
    far,
    own_sum,
    z_send,
    z_recv,
    last_send,
    last_recv,
    in_sem,
    w_sem,
    ssem,
    rsem,
    zs_sem,
    zr_sem,
):
    ra = lax.axis_index("ra")
    cb = lax.axis_index("cb")
    rows, width = xg.shape[2:]
    half = width // 2
    x_peer = (flip(ra, 1), cb)
    y_peer = (flip(ra, 2), cb)
    z_peers = [None] + [(flip(ra, 4 * k), cb) for k in range(1, planes)]
    core_peer = (ra, flip(cb, 1))
    halves = (pl.ds(0, half), pl.ds(half, half))
    first, second = halves

    barrier = pltpu.get_barrier_semaphore()
    peers = [x_peer, y_peer, core_peer] + z_peers[1:]
    for peer in peers:
        pl.semaphore_signal(barrier, inc=1, device_id=peer, device_id_type=MESH)
    own = pltpu.make_async_copy(x_hbm, xg.at[0, 0], in_sem.at[0])
    own.start()
    small = []
    for i, (src, dst) in enumerate(
        (
            (gain_hbm, gain_ref),
            (gate_scale_hbm, gate_scale_ref),
            (up_scale_hbm, up_scale_ref),
            (down_scale_hbm, down_scale_ref),
            (gain2_hbm, gain2_ref),
        )
    ):
        load = pltpu.make_async_copy(src, dst, in_sem.at[i + 1])
        load.start()
        small.append(load)
    loads = []
    for i, src in enumerate((gate_hbm, up_hbm, down_hbm)):
        load = pltpu.make_async_copy(src, wide.at[i], w_sem.at[i])
        load.start()
        loads.append(load)
    own.wait()
    pl.semaphore_wait(barrier, len(peers))

    copies = {}
    slots = []
    landed = {}
    idle = []
    early = list(range(ssem.shape[0]))

    def send(name, k, src, dst, peer):
        slot = len(slots)
        slots.append(name)
        landed[name, k] = rsem.at[slot]
        copy = pltpu.make_async_remote_copy(
            src_ref=src,
            dst_ref=dst,
            send_sem=idle.pop(0) if idle else ssem.at[early.pop(0)],
            recv_sem=rsem.at[slot],
            device_id=peer,
            device_id_type=MESH,
        )
        copy.start()
        copies[name, k] = copy

    seen = set()

    def arrived(name, k):
        if (name, k) in seen:
            return
        seen.add((name, k))
        copies[name, k].wait_recv()
        idle.append(landed[name, k])

    def to_x(k, h):
        send(("gx", h), k, xg.at[k, 0, :, halves[h]], xg.at[k, 1, :, halves[h]], x_peer)

    def to_y(k, h):
        send(("gy", h), k, xg.at[k, 0, :, halves[h]], xg.at[k, 2, :, halves[h]], y_peer)

    level = ra // 4
    inner = level % 2 != level // 2
    relays = []

    def to_z(source, target, h, peer):
        slot = len(relays)
        copy = pltpu.make_async_remote_copy(
            src_ref=xg.at[source, 0, :, halves[h]],
            dst_ref=xg.at[target, 0, :, halves[h]],
            send_sem=zs_sem.at[slot],
            recv_sem=zr_sem.at[target, h],
            device_id=z_peers[peer],
            device_id_type=MESH,
        )
        copies[("z", h), target] = copy
        landed[("z", h), target] = zr_sem.at[target, h]
        relays.append(copy)
        if source or peer != 1:
            pl.when(inner)(copy.start)
        else:
            copy.start()

    def at_z1(h):
        arrived(("z", h), 1)
        to_z(1, 2, h, 3)

    def pass_z2(h):
        arrived(("z", h), 2)
        to_z(2, 3, h, 1)

    def relay_z3(h):
        @pl.when(inner)
        def _():
            copies[("z", h), 3].wait_recv()

        to_z(3, 2, h, 1)

    def wait_z3(h):
        @pl.when(jnp.logical_not(inner))
        def _():
            copies[("z", h), 3].wait_recv()

    def across(h):
        arrived(("fx", "fy")[h], 0)
        send(("e", h), 1, xg.at[0, 3, :, halves[h]], xg.at[1, 3, :, halves[h]], z_peers[1])

    def forward_y(k):
        arrived(("gx", 1), k)
        send("fy", k, xg.at[k, 1, :, second], xg.at[k, 3, :, second], y_peer)

    def forward_x(k):
        arrived(("gy", 0), k)
        send("fx", k, xg.at[k, 2, :, first], xg.at[k, 3, :, first], x_peer)

    nt = (((1,), (1,)), ((), ()))

    def slot(k, s):
        if s == 1:
            arrived(("gx", 1), k)
            arrived(("gx", 0), k)
        elif s == 2:
            arrived(("gy", 0), k)
            arrived(("gy", 1), k)
        elif s == 3:
            for h in (1, 0):
                arrived(("e", h) if k == 1 else ("fx", "fy")[h], k)
        block = xg[k, s].astype(F32)
        total = jnp.sum(block * block, axis=1, keepdims=True)
        sq_send[k, s] = jnp.broadcast_to(total, (rows, 128))
        scaled[k, s] = (block * gain_ref[...]).astype(BF16)

    def squares(k):
        send("sq", k, sq_send.at[k], sq_recv.at[k], core_peer)

    def product(k, i):
        tokens = scaled[k].reshape(4 * rows, width)
        w = (gate_w, up_w)[i]
        product = lax.dot_general(tokens, w[...], nt, preferred_element_type=F32)
        part[k, i] = product
        ex_send[k, i] = product.astype(BF16)
        send(("ex", i), k, ex_send.at[k, i], ex_recv.at[k, i], core_peer)

    def activate(k):
        arrived("sq", k)
        arrived(("ex", 0), k)
        arrived(("ex", 1), k)
        for s in range(4):
            here = slice(s * rows, (s + 1) * rows)
            squares = (sq_send[k, s] + sq_recv[k, s])[:, :1]
            rscale = lax.rsqrt(squares / features + EPS)
            gate = (part[k, 0, here] + ex_recv[k, 0, here].astype(F32)) * rscale * gate_scale_ref[...][None, :]
            up = (part[k, 1, here] + ex_recv[k, 1, here].astype(F32)) * rscale * up_scale_ref[...][None, :]
            hidden[k, here] = (gate / (1.0 + jnp.exp(-gate)) * up).astype(BF16)

    def down_a(k):
        prod = jnp.dot(hidden[k], down_w[:, :half], preferred_element_type=F32)
        keep_a[k, 0] = prod[:rows]
        send_a[k, 0] = prod[rows : 2 * rows].astype(BF16)
        if k == 1:
            send2_a[k] = prod[2 * rows : 3 * rows].astype(BF16)
        else:
            keep_a[k, 1] = prod[2 * rows : 3 * rows]
        if k:
            send_a[k, 1] = prod[3 * rows :].astype(BF16)
        else:
            far[0] = prod[3 * rows :]

    def down_b(k):
        prod = jnp.dot(hidden[k], down_w[:, half:], preferred_element_type=F32)
        keep_b[k, 0] = prod[:rows]
        send_b[k, 0] = prod[2 * rows : 3 * rows].astype(BF16)
        if k == 1:
            send2_b[k] = prod[rows : 2 * rows].astype(BF16)
        else:
            keep_b[k, 1] = prod[rows : 2 * rows]
        if k:
            send_b[k, 1] = prod[3 * rows :].astype(BF16)
        else:
            far[1] = prod[3 * rows :]

    def one_a(k, d):
        send(("a1", d), k, send_a.at[k, d], recv_a.at[k, d], x_peer)

    def one_b(k, d):
        send(("b1", d), k, send_b.at[k, d], recv_b.at[k, d], y_peer)

    def send_r(h):
        src, dst = ((send_a, recv_a), (send_b, recv_b))[h]
        send(("r", h), 1, src.at[1, 1], dst.at[1, 1], z_peers[1])

    def pass_a():
        send("a2", 1, send2_a.at[1], recv2_a.at[1], y_peer)

    def pass_b():
        send("b2", 1, send2_b.at[1], recv2_b.at[1], x_peer)

    def merge_a():
        arrived(("r", 0), 1)
        send_a[0, 1] = (far[0] + recv_a[1, 1].astype(F32)).astype(BF16)
        one_a(0, 1)

    def merge_b():
        arrived(("r", 1), 1)
        send_b[0, 1] = (far[1] + recv_b[1, 1].astype(F32)).astype(BF16)
        one_b(0, 1)

    def two_a(k):
        arrived(("a1", 1), k)
        send2_a[k] = (keep_a[k, 1] + recv_a[k, 1].astype(F32)).astype(BF16)
        send("a2", k, send2_a.at[k], recv2_a.at[k], y_peer)

    def two_b(k):
        arrived(("b1", 1), k)
        send2_b[k] = (keep_b[k, 1] + recv_b[k, 1].astype(F32)).astype(BF16)
        send("b2", k, send2_b.at[k], recv2_b.at[k], x_peer)

    def home(k, h, mine):
        if k == 0:
            own_sum[:, halves[h]] = mine
            return
        if k == 3:
            arrived(("zs", h), 2)
            mine = mine + z_recv[2, h].astype(F32)
        peer = z_peers[1 if k == 2 else k]
        z_send[k, h] = mine.astype(BF16)
        send(("zs", h), k, z_send.at[k, h], z_recv.at[k, h], peer)

    def home_a(k):
        arrived(("a1", 0), k)
        arrived("a2", k)
        home(k, 0, keep_a[k, 0] + recv_a[k, 0].astype(F32) + recv2_a[k].astype(F32))

    def home_b(k):
        arrived(("b1", 0), k)
        arrived("b2", k)
        home(k, 1, keep_b[k, 0] + recv_b[k, 0].astype(F32) + recv2_b[k].astype(F32))

    def collect(k):
        for h in range(2):
            arrived(("zs", h), k)
            own_sum[:, halves[h]] += z_recv[k, h].astype(F32)

    def narrow(i, target):
        loads[i].wait()
        step = 64

        def body(j, carry):
            here = pl.ds(pl.multiple_of(j * step, step), step)
            target[here] = wide[i, here].astype(BF16)
            return carry

        lax.fori_loop(0, target.shape[0] // step, body, 0)

    for h in (1, 0):
        to_x(0, h)
        to_y(0, 1 - h)
        to_z(0, 1, h, 1)
    for h in (1, 0):
        to_z(0, 3, h, 3)
    for load in small:
        load.wait()
    slot(0, 0)
    narrow(1, up_w)
    narrow(0, gate_w)
    at_z1(1)
    forward_y(0)
    forward_x(0)
    relay_z3(1)
    narrow(2, down_w)
    at_z1(0)
    to_y(1, 0)
    to_y(1, 1)
    relay_z3(0)
    to_x(1, 0)
    to_x(1, 1)
    pass_z2(1)
    to_x(2, 1)
    pass_z2(0)
    across(0)
    slot(0, 3)
    slot(2, 0)
    slot(0, 2)
    to_y(2, 0)
    to_x(2, 0)
    slot(1, 2)
    to_y(2, 1)
    slot(0, 1)
    wait_z3(1)
    across(1)
    to_x(3, 1)
    product(0, 0)
    forward_y(2)
    wait_z3(0)
    forward_x(2)
    to_y(3, 0)
    slot(1, 1)
    slot(1, 0)
    product(0, 1)
    slot(2, 1)
    slot(2, 2)
    slot(1, 3)
    squares(1)
    product(1, 1)
    forward_y(3)
    product(1, 0)
    to_y(3, 1)
    to_x(3, 0)
    slot(2, 3)
    squares(2)
    product(2, 1)
    forward_x(3)
    product(2, 0)
    activate(1)
    down_a(1)
    squares(0)
    pass_a()
    one_a(1, 0)
    slot(3, 0)
    down_b(1)
    pass_b()
    activate(2)
    down_b(2)
    one_b(2, 1)
    slot(3, 1)
    send_r(1)
    down_a(2)
    one_a(2, 1)
    slot(3, 2)
    slot(3, 3)
    product(3, 0)
    one_b(1, 0)
    one_b(2, 0)
    squares(3)
    send_r(0)
    product(3, 1)
    two_b(2)
    one_a(2, 0)
    activate(3)
    home_a(1)
    down_b(3)
    one_b(3, 1)
    down_a(3)
    activate(0)
    home_b(1)
    two_a(2)
    down_b(0)
    one_a(3, 1)
    home_b(2)
    two_b(3)
    one_b(3, 0)
    one_a(3, 0)
    two_a(3)
    merge_b()
    home_a(2)
    down_a(0)
    one_b(0, 0)
    merge_a()
    home_b(3)
    one_a(0, 0)
    home_a(3)
    two_b(0)
    two_a(0)
    home_b(0)
    home_a(0)
    collect(1)
    collect(3)

    stream = 0.1 * xg[0, 0].astype(F32) + own_sum[...] * down_scale_ref[...]
    own_sum[...] = stream
    last_send[...] = jnp.broadcast_to(
        jnp.sum(stream * stream, axis=1, keepdims=True), last_send.shape
    )
    send("last", 0, last_send, last_recv, core_peer)
    arrived("last", 0)
    both = (last_send[...] + last_recv[...])[:, :1]
    rscale = lax.rsqrt(both / features + EPS)
    out_ref[...] = (own_sum[...] * rscale * gain2_ref[...]).astype(BF16)
    for (name, _), copy in copies.items():
        if name[0] != "z":
            copy.wait_send()
    for copy in relays[:2]:
        copy.wait_send()

    @pl.when(inner)
    def _():
        for copy in relays[2:]:
            copy.wait_send()


def fused(
    planes,
    activations,
    gain_first,
    gate_weight,
    gate_scale,
    up_weight,
    up_scale,
    down_weight,
    down_scale,
    gain_second,
):
    rows, width = activations.shape
    units = gate_weight.shape[0]
    half = width // 2
    group = 4 * rows
    n_copies = 17 * planes - 1
    vmem = pl.BlockSpec(memory_space=pltpu.VMEM)
    hbm = pl.BlockSpec(memory_space=pl.ANY)
    scratch = [
        pltpu.VMEM((3, units, width), F32),
        pltpu.VMEM((units, width), BF16),
        pltpu.VMEM((units, width), BF16),
        pltpu.VMEM((units, width), BF16),
        pltpu.VMEM((1, width), F32),
        pltpu.VMEM((units,), F32),
        pltpu.VMEM((units,), F32),
        pltpu.VMEM((1, width), F32),
        pltpu.VMEM((1, width), F32),
        pltpu.VMEM((planes, 4, rows, width), BF16),
        pltpu.VMEM((planes, 4, rows, width), BF16),
        pltpu.VMEM((planes, group, units), BF16),
        pltpu.VMEM((planes, 2, group, units), F32),
        pltpu.VMEM((planes, 2, group, units), BF16),
        pltpu.VMEM((planes, 2, group, units), BF16),
        pltpu.VMEM((planes, 4, rows, 128), F32),
        pltpu.VMEM((planes, 4, rows, 128), F32),
        pltpu.VMEM((planes, 2, rows, half), F32),
        pltpu.VMEM((planes, 2, rows, half), F32),
        pltpu.VMEM((planes, 2, rows, half), BF16),
        pltpu.VMEM((planes, 2, rows, half), BF16),
        pltpu.VMEM((planes, 2, rows, half), BF16),
        pltpu.VMEM((planes, 2, rows, half), BF16),
        pltpu.VMEM((planes, rows, half), BF16),
        pltpu.VMEM((planes, rows, half), BF16),
        pltpu.VMEM((planes, rows, half), BF16),
        pltpu.VMEM((planes, rows, half), BF16),
        pltpu.VMEM((2, rows, half), F32),
        pltpu.VMEM((rows, width), F32),
        pltpu.VMEM((planes, 2, rows, half), BF16),
        pltpu.VMEM((planes, 2, rows, half), BF16),
        pltpu.VMEM((rows, 128), F32),
        pltpu.VMEM((rows, 128), F32),
        pltpu.SemaphoreType.DMA((6,)),
        pltpu.SemaphoreType.DMA((3,)),
        pltpu.SemaphoreType.DMA((3 * planes,)),
        pltpu.SemaphoreType.DMA((n_copies,)),
        pltpu.SemaphoreType.DMA((10,)),
        pltpu.SemaphoreType.DMA((planes, 2)),
    ]
    return pl.pallas_call(
        functools.partial(kernel, planes, width * 2),
        out_shape=pltpu.VMEM((rows, width), BF16),
        in_specs=[hbm] * 9,
        out_specs=vmem,
        scratch_shapes=scratch,
        compiler_params=pltpu.CompilerParams(
            collective_id=0, has_side_effects=True, vmem_limit_bytes=60 * 1024 * 1024
        ),
    )(
        activations,
        gain_first[None, :],
        gate_weight,
        gate_scale,
        up_weight,
        up_scale,
        down_weight,
        down_scale[None, :],
        gain_second[None, :],
    )


def plain(
    activations,
    gain_first,
    gate_weight,
    gate_scale,
    up_weight,
    up_scale,
    down_weight,
    down_scale,
    gain_second,
):
    inputs = activations.astype(F32)
    features = activations.shape[1] * lax.axis_size("cb")
    gate_local = gate_weight.astype(BF16)
    up_local = up_weight.astype(BF16)
    down_local = down_weight.astype(BF16)
    gathered = lax.all_gather(activations, "ra", axis=0, tiled=True)
    wide_rows = gathered.astype(F32)
    row_squares = jnp.sum(wide_rows * wide_rows, axis=1)
    scaled = (wide_rows * gain_first).astype(BF16)
    contract = (((1,), (1,)), ((), ()))
    squares = lax.psum(row_squares, "cb")
    gate_part = lax.dot_general(gate_local, scaled, contract, preferred_element_type=F32)
    up_part = lax.dot_general(up_local, scaled, contract, preferred_element_type=F32)
    gate_sum, up_sum = lax.psum((gate_part, up_part), "cb")
    rscale_first = lax.rsqrt(squares / features + EPS)[None, :]
    gate_full = gate_sum * rscale_first * gate_scale[:, None]
    up_full = up_sum * rscale_first * up_scale[:, None]
    hidden = (jax.nn.silu(gate_full) * up_full).astype(BF16)
    mixed = lax.dot_general(hidden, down_local, (((0,), (0,)), ((), ())), preferred_element_type=F32)
    summed = lax.psum_scatter(mixed, "ra", scatter_dimension=0, tiled=True)
    stream = 0.1 * inputs + summed * down_scale
    second = lax.psum(jnp.sum(stream * stream, axis=1), "cb")
    rscale_second = lax.rsqrt(second / features + EPS)[:, None]
    return (stream * rscale_second * gain_second).astype(BF16)


def solution(mesh):
    placed = (
        P("ra", "cb"),
        P("cb"),
        P("ra", "cb"),
        P("ra"),
        P("ra", "cb"),
        P("ra"),
        P("ra", "cb"),
        P("cb"),
        P("cb"),
    )
    planes = mesh.shape["ra"] // 4
    paired = mesh.shape["cb"] == 2 and planes == 4
    body = functools.partial(fused, planes) if paired else plain
    return jax.shard_map(
        body, mesh=mesh, in_specs=placed, out_specs=P("ra", "cb"), check_vma=False
    )
```
